256 devices in a mesh: grp: 2 (over y), fs: 16 (over z), tp: 8 (over x, core).
Axes of the slice: x: 4, y: 2, z: 16, core: 2. Of those that a mesh axis runs over, the one named last changes fastest.
The devices are a block of a 4x16x16 slice.
Arguments:
- tokens: bfloat16 [8192, 2048], P(('grp', 'fs')), parts along dimension 0, may hold values from -6 to 6
- route_ids: int32 [8192, 2], P(('grp', 'fs')), parts along dimension 0, may hold values from 0 to 31, as said below
- route_weights: float32 [8192, 2], P(('grp', 'fs')), parts along dimension 0, may hold values from 0.2 to 1
- ffn_gain: float32 [2048], P('fs'), may hold values from 0.1 to 1.9
- gate_master: float32 [32, 2048, 1024], P(None, 'fs', 'tp'), may hold values from -0.125 to 0.125
- up_master: float32 [32, 2048, 1024], P(None, 'fs', 'tp'), may hold values from -0.125 to 0.125
- down_master: float32 [32, 1024, 2048], P(None, 'fs', 'tp'), may hold values from -0.1875 to 0.1875
Outputs:
- gate_serve: bfloat16 [64, 2048, 1024], P(('grp', 'fs'), None, 'tp'), parts along dimension 0
- up_serve: bfloat16 [64, 2048, 1024], P(('grp', 'fs'), None, 'tp'), parts along dimension 0
- down_serve: bfloat16 [64, 1024, 2048], P(('grp', 'fs'), None, 'tp'), parts along dimension 0
- mixed: bfloat16 [8192, 2048], P(('grp', 'fs'), 'tp'), parts along dimension 0
The draws below stay inside these ranges and needn't reach their ends.
There are 2 independent parts, one for each index of `grp`. The reference program is written for one: setup_inputs(seed, part) draws one part's arguments, and reference() takes and returns one part's arrays. A program takes and returns all parts, laid end to end along the dimension named above; an argument that names none is the same for every part. Nothing has to cross between parts.
Inputs may be any that keep to these rules, and one draw needn't show every extreme that they name: `route_ids`: each row names two different experts of one group of 8 consecutive experts. Among the tokens of one index of fs, each group is named by exactly 64 tokens and no expert by more than 32; in every group one expert, the same for every index of fs, is named by exactly 32, and so is one other expert of the group, which may change from one index of fs to the next.
All inputs are finite; a program needn't handle non-finite values.
Results may differ from the reference program's by a relative error of at most 0.0087.
Values may be sent and summed in bfloat16 or wider, within the bound.
No kernel may reach another device: no remote copies, remote signals or barrier semaphores. Data moves between devices by JAX's collectives and lax.ppermute only.
A program may use at most 64 MiB of HBM per device.

```python
import jax
import jax.numpy as jnp
from jax import lax

D = 2048
FF = 1024
GROUP_SIZE = 8
TOK_DEV = 256
EXPERTS = 32
GROUPS = 4
CAP = 32
TOKENS = 4096
N_FS = 16


def draw_route_ids(key, part):
    blocks = TOKENS // TOK_DEV
    per_group = TOK_DEV // GROUPS
    half_group = per_group // 2
    others_count = GROUP_SIZE - 2
    hot_local = jax.random.randint(jax.random.fold_in(key, 11), (GROUPS,), 0, GROUP_SIZE).astype(jnp.int32)
    rank_list = jnp.arange(TOK_DEV, dtype=jnp.int32)
    group_of = rank_list // per_group
    within = rank_list % per_group
    leading = within < half_group
    local_list = jnp.arange(GROUP_SIZE, dtype=jnp.int32)
    block_keys = jax.random.split(jax.random.fold_in(key, 13), blocks)
    block_list = jnp.arange(blocks, dtype=jnp.int32)

    def one_block(subkey, block_index):
        step_draw = jax.random.randint(jax.random.fold_in(subkey, 4), (GROUPS,), 0, GROUP_SIZE - 1).astype(jnp.int32)
        drawn_second = (hot_local + 1 + step_draw) % GROUP_SIZE
        paired = jnp.bitwise_xor(hot_local, 1)
        second_full = jnp.where(block_index % 2 == 0, paired, drawn_second)
        group_keys = jax.random.split(jax.random.fold_in(subkey, 3), GROUPS)
        ranks = jax.vmap(lambda inner_key: jax.random.permutation(inner_key, GROUP_SIZE))(group_keys).astype(jnp.int32)
        excluded = (local_list[None, :] == hot_local[:, None]) | (local_list[None, :] == second_full[:, None])
        scores = ranks + GROUP_SIZE * excluded.astype(jnp.int32)
        ordered = jnp.argsort(scores, axis=1).astype(jnp.int32)
        others = ordered[:, :others_count]
        first_local = jnp.where(leading, hot_local[group_of], second_full[group_of])
        second_local = others[group_of, within % others_count]
        pairing = jnp.stack([first_local, second_local], axis=1) + group_of[:, None] * GROUP_SIZE
        placing = jax.random.permutation(jax.random.fold_in(subkey, 1), TOK_DEV)
        flipped = jax.random.randint(jax.random.fold_in(subkey, 2), (TOK_DEV, 1), 0, 2)
        swapped = jnp.where(flipped == 1, pairing[:, ::-1], pairing)
        return jnp.zeros((TOK_DEV, 2), jnp.int32).at[placing].set(swapped.astype(jnp.int32))
    return jax.vmap(one_block)(block_keys, block_list).reshape(TOKENS, 2).astype(jnp.int32)


def shard_levels(key, extent, cuts, low, largest):
    def one(axis_at, shards_of):
        heights = jax.random.uniform(jax.random.fold_in(jax.random.fold_in(key, 6), axis_at), (shards_of,), jnp.float32, low / len(cuts), largest / len(cuts))
        return jnp.repeat(jnp.exp(heights), extent[axis_at] // shards_of).reshape((-1,) + (1,) * (len(extent) - axis_at - 1))

    factor_of = one(*cuts[0])
    for cut in cuts[1:]:
        factor_of = factor_of * one(*cut)
    return factor_of


def normal_values(key, dims, scale, limit, cuts=(), held_as=jnp.bfloat16):
    entries = jax.random.normal(key, dims, jnp.float32) * scale
    if len(cuts) > 0:
        entries = shard_levels(key, dims, cuts, -0.22, 0.18) * entries
    return jnp.clip(entries, min=-limit, max=limit).astype(held_as)


def setup_inputs(seed: int = 0, part: int = 0) -> dict:
    key_list = jax.random.split(jax.random.key(seed), 8)
    part_splits = jax.random.split(jax.random.fold_in(key_list[7], part), 8)
    tokens = normal_values(part_splits[0], (TOKENS, D), 1.0, 6.0, ((0, 16),))
    route_ids = draw_route_ids(jax.random.fold_in(jax.random.fold_in(key_list[7], part), 71), part)
    route_weights = jnp.clip(0.2 + 0.8 * jax.random.uniform(part_splits[2], (TOKENS, 2), jnp.float32) ** shard_levels(part_splits[2], (TOKENS, 2), ((0, 16),), -0.2, 0.2), 0.2, 1.0)
    ffn_gain = jnp.clip(1.0 + 0.18 * jax.random.normal(key_list[3], (D,), jnp.float32), 0.1, 1.9)
    gate_master = normal_values(key_list[4], (EXPERTS, D, FF), D ** -0.5, 0.125, ((1, 16), (2, 8)), jnp.float32)
    up_master = normal_values(key_list[5], (EXPERTS, D, FF), D ** -0.5, 0.125, ((1, 16), (2, 8)), jnp.float32)
    down_master = normal_values(key_list[6], (EXPERTS, FF, D), FF ** -0.5, 0.1875, ((1, 16), (2, 8)), jnp.float32)
    return {"tokens": tokens, "route_ids": route_ids, "route_weights": route_weights, "ffn_gain": ffn_gain, "gate_master": gate_master, "up_master": up_master, "down_master": down_master}


def reference(tokens, route_ids, route_weights, ffn_gain, gate_master, up_master, down_master):
    row_gain = ffn_gain.astype(jnp.float32)[None, :, None]
    gate_serve = (gate_master * row_gain).astype(jnp.bfloat16)
    up_serve = (up_master * row_gain).astype(jnp.bfloat16)
    down_serve = down_master.astype(jnp.bfloat16)
    token_rows = tokens.astype(jnp.float32)
    normed = (token_rows * lax.rsqrt(lax.optimization_barrier(jnp.mean(token_rows * token_rows, axis=1, keepdims=True)) + 1e-06)).astype(jnp.bfloat16)
    flat_ids = route_ids.reshape(-1).astype(jnp.int32)
    flat_weights = route_weights.reshape(-1).astype(jnp.float32)
    slot_limit = N_FS * CAP

    def one_expert(inputs):
        expert, w_gate, w_up, w_down = inputs
        matches = flat_ids == expert
        chosen = jnp.nonzero(matches, size=slot_limit, fill_value=0)[0].astype(jnp.int32)
        live_count = jnp.sum(matches.astype(jnp.int32))
        is_live = jnp.arange(slot_limit, dtype=jnp.int32) < live_count
        picked = normed[chosen // 2]
        gate_val = jnp.dot(picked, w_gate, preferred_element_type=jnp.float32)
        up_val = jnp.dot(picked, w_up, preferred_element_type=jnp.float32)
        hidden = (jax.nn.silu(gate_val) * up_val).astype(jnp.bfloat16)
        route_out = jnp.dot(hidden, w_down, preferred_element_type=jnp.float32).astype(jnp.bfloat16)
        route_scale = jnp.where(is_live, flat_weights[chosen], jnp.zeros_like(flat_weights[chosen]))
        return (chosen // 2, route_out.astype(jnp.float32) * route_scale[:, None])
    expert_list = jnp.arange(gate_serve.shape[0], dtype=jnp.int32)
    owners, terms = lax.map(one_expert, (expert_list, gate_serve, up_serve, down_serve))
    combined = jnp.zeros(tokens.shape, jnp.float32).at[owners.reshape(-1)].add(terms.reshape(-1, tokens.shape[1]))
    return (gate_serve, up_serve, down_serve, combined.astype(jnp.bfloat16))
```

```python
import jax
import jax.numpy as jnp
from jax import lax
from jax.experimental import pallas as pl
from jax.experimental.pallas import tpu as pltpu
from jax.sharding import Mesh
from jax.sharding import PartitionSpec as P

GROUP_SIZE = 8
FS = ("fh", "fl")
TP = ("tp_0", "tp_1")
META = 8
BF = jnp.bfloat16
F32 = jnp.float32

VM = pl.BlockSpec(memory_space=pltpu.VMEM)
SM = pl.BlockSpec(memory_space=pltpu.SMEM)


def shift(x, axis, k):
    n = lax.axis_size(axis)
    return lax.ppermute(x, axis, [(i, (i + k) % n) for i in range(n)])


def call(body, out_shape, *args, specs):
    return pl.pallas_call(
        body,
        out_shape=out_shape,
        in_specs=list(specs),
        out_specs=jax.tree.map(lambda _: VM, out_shape),
    )(*args)


def shape(dims, dtype=BF):
    return jax.ShapeDtypeStruct(dims, dtype)


def iota(dims, dim):
    return lax.broadcasted_iota(jnp.int32, dims, dim)


def dot(a, b, dims=((1,), (0,))):
    return lax.dot_general(a, b, (dims, ((), ())), preferred_element_type=F32)


def prep_tokens(tokens, route_ids, route_weights, places, groups, width):
    rows, _ = tokens.shape
    part = rows // groups

    def body(places_ref, tok_ref, ids_ref, w_ref, out_ref, order_ref):
        tok = tok_ref[...].astype(F32)
        scale = lax.rsqrt(jnp.mean(tok * tok, axis=1, keepdims=True) + 1e-06)
        own = tok_ref[:, pl.ds(pl.multiple_of(places_ref[1] * width, width), width)].astype(F32)
        own = (own * scale).astype(BF)
        ids = ids_ref[...]
        group = ids[:, 0:1] // GROUP_SIZE
        far = group - places_ref[0]
        far = jnp.where(far < 0, far + groups, far)
        member = (iota((rows, 128), 1) == far).astype(F32)
        before = (iota((rows, rows), 0) > iota((rows, rows), 1)).astype(BF)
        rank = jnp.sum(dot(before, member.astype(BF)) * member, axis=1, keepdims=True)
        place = far * part + rank.astype(jnp.int32)
        order = (iota((rows, rows), 1) == place).astype(BF)
        order_ref[...] = order
        ordered = dot(order, own, ((0,), (0,))).astype(BF)
        first = (ids[:, 0:1] - group * GROUP_SIZE).astype(F32)
        second = (ids[:, 1:2] - group * GROUP_SIZE).astype(F32)
        w = w_ref[...]
        w0, w1 = (w[:, 0:1], w[:, 1:2])
        h0, h1 = (w0.astype(BF).astype(F32), w1.astype(BF).astype(F32))
        meta = jnp.concatenate(
            [
                jnp.sum(order.astype(F32) * v, axis=0, keepdims=True)
                for v in (first, second, h0, w0 - h0, h1, w1 - h1, first * 0.0, first * 0.0)
            ],
            axis=0,
        )
        for k in range(groups):
            out_ref[k, :part, :] = ordered[k * part : (k + 1) * part]
            piece = meta[:, k * part : (k + 1) * part]
            piece = jnp.concatenate([piece, jnp.zeros((META, width - part), F32)], axis=1)
            out_ref[k, part:, :] = piece.astype(BF)

    return call(
        body,
        (shape((groups, part + META, width)), shape((rows, rows))),
        places,
        tokens,
        route_ids,
        route_weights,
        specs=(SM, VM, VM, VM),
    )


def select_rows(blocks, places, per_device, capacity):
    lo = len(blocks)
    hi, rows, width = blocks[0].shape
    part = rows - META
    sources = lo * hi
    slots = per_device * capacity

    def body(places_ref, *refs):
        ins, (out_ref, back_ref) = (refs[:lo], refs[lo:])
        metas = [ins[c][k, part:, :part].astype(F32) for c in range(lo) for k in range(hi)]
        row = [jnp.concatenate([m[r : r + 1] for m in metas], axis=0) for r in range(6)]
        earlier = (iota((part, part), 0) < iota((part, part), 1)).astype(BF)
        slot = iota((capacity, part), 0).astype(F32)
        base = (places_ref[2] * per_device).astype(F32)
        member, rank, high, low = ([], [], [], [])
        for e in range(per_device):
            one, two = (row[0] == base + e, row[1] == base + e)
            m = jnp.where(one | two, 1.0, 0.0)
            member.append(m)
            rank.append(jnp.where(one | two, dot(m.astype(BF), earlier), -1.0))
            high.append(jnp.where(one, row[2], 0.0) + jnp.where(two, row[4], 0.0))
            low.append(jnp.where(one, row[3], 0.0) + jnp.where(two, row[5], 0.0))
        for j in range(sources):
            pick = [(slot == rank[e][j : j + 1]).astype(F32) for e in range(per_device)]
            both = jnp.concatenate(pick, axis=0).astype(BF)
            got = dot(both, ins[j // hi][j % hi, :part, :]).astype(BF)
            for e in range(per_device):
                out_ref[e, j * capacity : (j + 1) * capacity, :] = got[e * capacity : (e + 1) * capacity]
            weighted = [pick[e] * high[e][j : j + 1] for e in range(per_device)]
            weighted += [pick[e] * low[e][j : j + 1] for e in range(per_device)]
            back_ref[j] = jnp.concatenate(weighted, axis=0).astype(BF)

    return call(
        body,
        (shape((per_device, sources * capacity, width)), shape((sources, 2 * slots, part))),
        places,
        *blocks,
        specs=(SM,) + (VM,) * lo,
    )


def gather_tp(x):
    half = x.shape[1] // 2
    left, right = (shift(x, "tp_0", 1), shift(x, "tp_0", -1))
    across = (shift(left[:, :half], "tp_0", 1), shift(right[:, half:], "tp_0", -1))
    mine = (x, left, right, *across)
    return mine + tuple(shift(b, "tp_1", 1) for b in mine)


def blocks_of(refs, places_ref):
    for c in range(2):
        core = places_ref[4] if c == 0 else 1 - places_ref[4]
        for at, back in ((0, 0), (1, 3), (2, 1), (3, 2), (4, 2)):
            x = (places_ref[3] + back) % 4
            yield refs[5 * c + at], x * 2 + core, at


def first_matmuls(blocks, gate, up, places):
    per_device, rows, width = blocks[0].shape
    cols = gate.shape[2]
    half = rows // 2

    def body(places_ref, *refs):
        ins, (gate_ref, up_ref, out_ref, acc_ref) = (refs[:10], refs[10:])
        for e in range(per_device):
            acc_ref[...] = jnp.zeros((rows, 2 * cols), F32)
            for ref, tp, at in blocks_of(ins, places_ref):
                d = pl.ds(pl.multiple_of(tp * width, width), width)
                w = jnp.concatenate([gate_ref[e, d, :], up_ref[e, d, :]], axis=1)
                to = slice(0, half) if at == 3 else slice(half, rows) if at == 4 else slice(0, rows)
                acc_ref[to, :] += dot(ref[e], w)
            g = acc_ref[:, :cols]
            out_ref[e] = (g / (1.0 + jnp.exp(-g)) * acc_ref[:, cols:]).astype(BF)

    return pl.pallas_call(
        body,
        out_shape=shape((per_device, rows, cols)),
        in_specs=[SM] + [VM] * 12,
        out_specs=VM,
        scratch_shapes=[pltpu.VMEM((rows, 2 * cols), F32)],
    )(places, *blocks, gate, up)


def second_matmul(blocks, down, back, places, lo, hi, part):
    per_device, rows, width = blocks[0].shape
    cols = down.shape[2]
    half = rows // 2
    sources = lo * hi
    capacity = rows // sources

    def body(places_ref, *refs):
        ins, (down_ref, back_ref) = (refs[:10], refs[10:12])
        outs, (acc_ref, row_ref) = (refs[12 : 12 + lo], refs[12 + lo :])
        for e in range(per_device):
            acc_ref[...] = jnp.zeros((rows, cols), F32)
            for ref, tp, at in blocks_of(ins, places_ref):
                w = down_ref[e, pl.ds(pl.multiple_of(tp * width, width), width), :]
                to = slice(0, half) if at == 3 else slice(half, rows) if at == 4 else slice(0, rows)
                acc_ref[to, :] += dot(ref[e], w)
            row_ref[e] = acc_ref[...].astype(BF)
        for j in range(sources):
            own = [row_ref[e, j * capacity : (j + 1) * capacity, :] for e in range(per_device)]
            own = jnp.concatenate(own + own, axis=0)
            outs[j // hi][j % hi] = dot(back_ref[j], own, ((0,), (0,))).astype(BF)

    return pl.pallas_call(
        body,
        out_shape=tuple(shape((hi, part, cols)) for _ in range(lo)),
        in_specs=[SM] + [VM] * 12,
        out_specs=tuple(VM for _ in range(lo)),
        scratch_shapes=[pltpu.VMEM((rows, cols), F32), pltpu.VMEM((per_device, rows, cols), BF)],
    )(places, *blocks, down, back)


def put_in_order(order, parts):
    rows = order.shape[0]
    part, cols = parts[0].shape

    def body(order_ref, *refs):
        both = jnp.concatenate([r[...] for r in refs[:-1]], axis=0)
        refs[-1][...] = dot(order_ref[...], both).astype(BF)

    return call(body, shape((rows, cols)), order, *parts, specs=(VM,) * (1 + len(parts)))


def share(master, index, count, n):
    experts, rows, cols = master.shape
    per_device = experts // n
    whole = per_device * rows
    return lax.dynamic_slice_in_dim(
        master.reshape(n, whole, cols), index * (whole // count), whole // count, 1
    )


def ring(x, axis):
    n = lax.axis_size(axis)
    out, ahead, behind = ([(0, x)], x, x)
    for k in range(1, n // 2 + 1):
        ahead = shift(ahead, axis, 1)
        out.append((k, ahead))
        if k <= (n - 1) // 2:
            behind = shift(behind, axis, -1)
            out.append((n - k, behind))
    return out


def assemble(pieces, index, count, per_device):
    n, rows, cols = pieces[0][1].shape
    buffer = jnp.zeros((count, n, rows, cols), BF)
    for back, piece in pieces:
        at = (index - back) % count
        buffer = lax.dynamic_update_slice(buffer, piece[None], (at, 0, 0, 0))
    split = count // per_device
    buffer = buffer.reshape(per_device, split, n, rows, cols).transpose(0, 2, 1, 3, 4)
    return buffer.reshape(per_device, -1, cols)


def on_device(tokens, route_ids, route_weights, ffn_gain, gate_master, up_master, down_master):
    n = lax.axis_size(FS)
    hi, lo = (lax.axis_size("fh"), lax.axis_size("fl"))
    count, index = (lax.axis_size("grp"), lax.axis_index("grp"))
    experts = gate_master.shape[0]
    per_device = experts // n
    width = tokens.shape[1] // lax.axis_size(TP)
    capacity = tokens.shape[0] // (2 * hi)
    part = tokens.shape[0] // hi
    places = jnp.stack(
        [
            lax.axis_index("fh"),
            lax.axis_index(TP),
            lax.axis_index("fl"),
            lax.axis_index("tp_0"),
            lax.axis_index("tp_1"),
        ]
    ).astype(jnp.int32)

    def swap(x):
        return lax.all_to_all(x, FS, split_axis=0, concat_axis=0, tiled=True)

    with jax.named_scope("weights"):
        gate_share = share(gate_master, index, count, n)
        up_share = share(up_master, index, count, n)
        down_share = share(down_master, index, count, n).astype(BF)
        size = gate_share.shape[1]
        gain = jnp.concatenate([ffn_gain] * per_device)
        gain = lax.dynamic_slice_in_dim(gain, index * size, size)[None, :, None]
        both = jnp.concatenate([(gate_share * gain).astype(BF), (up_share * gain).astype(BF)], axis=1)
        both = swap(both)

    with jax.named_scope("tokens"):
        sent, order = prep_tokens(tokens, route_ids, route_weights, places, hi, width)
        near = jnp.stack([sent[0]] + [shift(sent[k], "fh", k) for k in range(1, hi)])
        blocks = [near] + [shift(near, "fl", k) for k in range(1, lo)]
        portion, back = select_rows(blocks, places, per_device, capacity)
        rows = gather_tp(portion)

    with jax.named_scope("down"):
        down = swap(down_share)
    with jax.named_scope("exchange"):
        pieces = ring(both, "grp")
        gate_serve = assemble([(k, p[:, :size]) for k, p in pieces], index, count, per_device)
        up_serve = assemble([(k, p[:, size:]) for k, p in pieces], index, count, per_device)
        down_serve = assemble(ring(down, "grp"), index, count, per_device)

    with jax.named_scope("experts"):
        hidden = gather_tp(first_matmuls(rows, gate_serve, up_serve, places))
        sums = second_matmul(hidden, down_serve, back, places, lo, hi, part)
    with jax.named_scope("home"):
        total = sums[0].astype(F32)
        for k in range(1, lo):
            total = total + shift(sums[k], "fl", -k).astype(F32)
        total = total.astype(BF)
        parts = [total[0]] + [shift(total[k], "fh", -k) for k in range(1, hi)]
        mixed = put_in_order(order, parts)
    return (gate_serve, up_serve, down_serve, mixed)


def solution(mesh):
    grp, fs, tp = (mesh.shape["grp"], mesh.shape["fs"], mesh.shape["tp"])

    def build(*args):
        per_device = args[4].shape[0] // fs
        members = GROUP_SIZE // per_device
        split = Mesh(
            mesh.devices.reshape(grp, fs // members, members, tp // 2, 2),
            ("grp", "fh", "fl", "tp_0", "tp_1"),
        )
        in_specs = (
            P(("grp", *FS), None),
            P(("grp", *FS), None),
            P(("grp", *FS), None),
            P(FS),
            P(None, FS, TP),
            P(None, FS, TP),
            P(None, FS, TP),
        )
        out_specs = (
            P(("grp", *FS), None, TP),
            P(("grp", *FS), None, TP),
            P(("grp", *FS), None, TP),
            P(("grp", *FS), TP),
        )
        return jax.shard_map(
            on_device, mesh=split, in_specs=in_specs, out_specs=out_specs, check_vma=False
        )(*args)

    return build
```

```python
import jax
import jax.numpy as jnp
from jax import lax
from jax.experimental import pallas as pl
from jax.experimental.pallas import tpu as pltpu
from jax.sharding import Mesh
from jax.sharding import PartitionSpec as P


GROUP_SIZE = 8
FS = ("fh", "fl")
TP = ("tp_0", "tp_1")
META = 8
BF = jnp.bfloat16
F32 = jnp.float32

VM = pl.BlockSpec(memory_space=pltpu.VMEM)
SM = pl.BlockSpec(memory_space=pltpu.SMEM)


def shift(x, axis, k):
    n = lax.axis_size(axis)
    return lax.ppermute(x, axis, [(i, (i + k) % n) for i in range(n)])


def call(body, out_shape, *args, specs):
    return pl.pallas_call(
        body,
        out_shape=out_shape,
        in_specs=list(specs),
        out_specs=jax.tree.map(lambda _: VM, out_shape),
    )(*args)


def shape(dims, dtype=BF):
    return jax.ShapeDtypeStruct(dims, dtype)


def iota(dims, dim):
    return lax.broadcasted_iota(jnp.int32, dims, dim)


def dot(a, b, dims=((1,), (0,))):
    return lax.dot_general(a, b, (dims, ((), ())), preferred_element_type=F32)


def prep_tokens(tokens, route_ids, places, groups, width):
    rows, _ = tokens.shape
    part = rows // groups

    def body(places_ref, tok_ref, ids_ref, out_ref):
        tok = tok_ref[...].astype(F32)
        scale = lax.rsqrt(jnp.mean(tok * tok, axis=1, keepdims=True) + 1e-06)
        own = tok_ref[:, pl.ds(pl.multiple_of(places_ref[1] * width, width), width)].astype(F32)
        own = (own * scale).astype(BF)
        ids = ids_ref[...]
        group = ids[:, 0:1] // GROUP_SIZE
        far = group - places_ref[0]
        far = jnp.where(far < 0, far + groups, far)
        member = (iota((rows, 128), 1) == far).astype(F32)
        before = (iota((rows, rows), 0) > iota((rows, rows), 1)).astype(BF)
        rank = jnp.sum(dot(before, member.astype(BF)) * member, axis=1, keepdims=True)
        place = far * part + rank.astype(jnp.int32)
        order = (iota((rows, rows), 1) == place).astype(BF)
        ordered = dot(order, own, ((0,), (0,))).astype(BF)
        first = (ids[:, 0:1] - group * GROUP_SIZE).astype(F32)
        second = (ids[:, 1:2] - group * GROUP_SIZE).astype(F32)
        meta = jnp.concatenate(
            [
                jnp.sum(order.astype(F32) * v, axis=0, keepdims=True)
                for v in (first, second)
            ]
            + [jnp.zeros((META - 2, rows), F32)],
            axis=0,
        )
        for k in range(groups):
            out_ref[k, :part, :] = ordered[k * part : (k + 1) * part]
            piece = meta[:, k * part : (k + 1) * part]
            piece = jnp.concatenate([piece, jnp.zeros((META, width - part), F32)], axis=1)
            out_ref[k, part:, :] = piece.astype(BF)

    return call(
        body,
        shape((groups, part + META, width)),
        places,
        tokens,
        route_ids,
        specs=(SM, VM, VM),
    )


def select_rows(blocks, places, per_device, capacity):
    lo = len(blocks)
    hi, rows, width = blocks[0].shape
    part = rows - META
    sources = lo * hi

    def body(places_ref, *refs):
        ins, out_ref = (refs[:lo], refs[lo])
        metas = [ins[c][k, part:, :part].astype(F32) for c in range(lo) for k in range(hi)]
        row = [jnp.concatenate([m[r : r + 1] for m in metas], axis=0) for r in range(2)]
        earlier = (iota((part, part), 0) < iota((part, part), 1)).astype(BF)
        slot = iota((capacity, part), 0).astype(F32)
        base = (places_ref[2] * per_device).astype(F32)
        rank = []
        for e in range(per_device):
            one, two = (row[0] == base + e, row[1] == base + e)
            m = jnp.where(one | two, 1.0, 0.0)
            rank.append(jnp.where(one | two, dot(m.astype(BF), earlier), -1.0))
        for j in range(sources):
            pick = [(slot == rank[e][j : j + 1]).astype(F32) for e in range(per_device)]
            both = jnp.concatenate(pick, axis=0).astype(BF)
            got = dot(both, ins[j // hi][j % hi, :part, :]).astype(BF)
            for e in range(per_device):
                out_ref[e, j * capacity : (j + 1) * capacity, :] = got[e * capacity : (e + 1) * capacity]

    return call(
        body,
        shape((per_device, sources * capacity, width)),
        places,
        *blocks,
        specs=(SM,) + (VM,) * lo,
    )


def gather_tp(x):
    half = x.shape[1] // 2
    left, right = (shift(x, "tp_0", 1), shift(x, "tp_0", -1))
    across = (shift(left[:, :half], "tp_0", 1), shift(right[:, half:], "tp_0", -1))
    mine = (x, left, right, *across)
    return mine + tuple(shift(b, "tp_1", 1) for b in mine)


def blocks_of(refs, places_ref):
    for c in range(2):
        core = places_ref[4] if c == 0 else 1 - places_ref[4]
        for at, back in ((0, 0), (1, 3), (2, 1), (3, 2), (4, 2)):
            x = (places_ref[3] + back) % 4
            yield refs[5 * c + at], x * 2 + core, at


def first_matmuls(blocks, gate, up, places):
    per_device, rows, width = blocks[0].shape
    cols = gate.shape[2]
    half = rows // 2

    def body(places_ref, *refs):
        ins, (gate_ref, up_ref, out_ref, acc_ref) = (refs[:10], refs[10:])
        for e in range(per_device):
            acc_ref[...] = jnp.zeros((rows, 2 * cols), F32)
            for ref, tp, at in blocks_of(ins, places_ref):
                d = pl.ds(pl.multiple_of(tp * width, width), width)
                w = jnp.concatenate([gate_ref[e, d, :], up_ref[e, d, :]], axis=1)
                to = slice(0, half) if at == 3 else slice(half, rows) if at == 4 else slice(0, rows)
                acc_ref[to, :] += dot(ref[e], w)
            g = acc_ref[:, :cols]
            out_ref[e] = (g / (1.0 + jnp.exp(-g)) * acc_ref[:, cols:]).astype(BF)

    return pl.pallas_call(
        body,
        out_shape=shape((per_device, rows, cols)),
        in_specs=[SM] + [VM] * 12,
        out_specs=VM,
        scratch_shapes=[pltpu.VMEM((rows, 2 * cols), F32)],
    )(places, *blocks, gate, up)


def second_matmul(blocks, down, places, lo, hi):
    per_device, rows, width = blocks[0].shape
    cols = down.shape[2]
    half = rows // 2
    sources = lo * hi
    capacity = rows // sources

    def body(places_ref, *refs):
        ins, (down_ref, out_ref, acc_ref) = (refs[:10], refs[10:])
        for e in range(per_device):
            acc_ref[...] = jnp.zeros((rows, cols), F32)
            for ref, tp, at in blocks_of(ins, places_ref):
                w = down_ref[e, pl.ds(pl.multiple_of(tp * width, width), width), :]
                to = slice(0, half) if at == 3 else slice(half, rows) if at == 4 else slice(0, rows)
                acc_ref[to, :] += dot(ref[e], w)
            for j in range(sources):
                fh, fl = (places_ref[0] - j % hi, places_ref[2] - j // hi)
                fh, fl = (jnp.where(fh < 0, fh + hi, fh), jnp.where(fl < 0, fl + lo, fl))
                out_ref[fh * lo + fl, e] = acc_ref[j * capacity : (j + 1) * capacity, :].astype(BF)

    return pl.pallas_call(
        body,
        out_shape=shape((sources, per_device, capacity, cols)),
        in_specs=[SM] + [VM] * 11,
        out_specs=VM,
        scratch_shapes=[pltpu.VMEM((rows, cols), F32)],
    )(places, *blocks, down)


def combine(returned, route_ids, route_weights, capacity):
    rows, cols = (route_ids.shape[0], returned.shape[1])
    slots = returned.shape[0]

    def body(ret_ref, ids_ref, w_ref, out_ref):
        ids, w = (ids_ref[...], w_ref[...])
        lane = iota((rows, 128), 1)
        one, two = (lane == ids[:, 0:1], lane == ids[:, 1:2])
        before = (iota((rows, rows), 0) > iota((rows, rows), 1)).astype(BF)
        count = dot(before, jnp.where(one | two, 1.0, 0.0).astype(BF))
        total = jnp.zeros((rows, cols), F32)
        for r, hit in ((0, one), (1, two)):
            rank = jnp.sum(jnp.where(hit, count, 0.0), axis=1, keepdims=True).astype(jnp.int32)
            pick = (iota((rows, slots), 1) == ids[:, r : r + 1] * capacity + rank).astype(BF)
            total = total + dot(pick, ret_ref[...]) * w[:, r : r + 1]
        out_ref[...] = total.astype(BF)

    return call(body, shape((rows, cols)), returned, route_ids, route_weights, specs=(VM,) * 3)


def share(master, index, count, n):
    experts, rows, cols = master.shape
    per_device = experts // n
    whole = per_device * rows
    return lax.dynamic_slice_in_dim(
        master.reshape(n, whole, cols), index * (whole // count), whole // count, 1
    )


def ring(x, axis):
    n = lax.axis_size(axis)
    out, ahead, behind = ([(0, x)], x, x)
    for k in range(1, n // 2 + 1):
        ahead = shift(ahead, axis, 1)
        out.append((k, ahead))
        if k <= (n - 1) // 2:
            behind = shift(behind, axis, -1)
            out.append((n - k, behind))
    return out


def assemble(pieces, index, count, per_device):
    n, rows, cols = pieces[0][1].shape
    buffer = jnp.zeros((count, n, rows, cols), BF)
    for back, piece in pieces:
        at = (index - back) % count
        buffer = lax.dynamic_update_slice(buffer, piece[None], (at, 0, 0, 0))
    split = count // per_device
    buffer = buffer.reshape(per_device, split, n, rows, cols).transpose(0, 2, 1, 3, 4)
    return buffer.reshape(per_device, -1, cols)


def on_device(tokens, route_ids, route_weights, ffn_gain, gate_master, up_master, down_master):
    n = lax.axis_size(FS)
    hi, lo = (lax.axis_size("fh"), lax.axis_size("fl"))
    count, index = (lax.axis_size("grp"), lax.axis_index("grp"))
    experts = gate_master.shape[0]
    per_device = experts // n
    width = tokens.shape[1] // lax.axis_size(TP)
    capacity = tokens.shape[0] // (2 * hi)
    places = jnp.stack(
        [
            lax.axis_index("fh"),
            lax.axis_index(TP),
            lax.axis_index("fl"),
            lax.axis_index("tp_0"),
            lax.axis_index("tp_1"),
        ]
    ).astype(jnp.int32)

    def swap(x):
        return lax.all_to_all(x, FS, split_axis=0, concat_axis=0, tiled=True)

    rows = gate_master.shape[1]
    size = per_device * rows // count
    if size < rows:
        gain = lax.dynamic_slice_in_dim(ffn_gain, index * size % rows, size)
    else:
        gain = jnp.concatenate([ffn_gain] * (size // rows))
    gain = gain[None, :, None]

    gate = swap((share(gate_master, index, count, n) * gain).astype(BF))
    sent = prep_tokens(tokens, route_ids, places, hi, width)
    far = [shift(sent[k], "fh", k) for k in range(1, hi)]
    near = jnp.stack([sent[0]] + far)
    up = swap((share(up_master, index, count, n) * gain).astype(BF))
    blocks = [near] + [shift(near, "fl", k) for k in range(1, lo)]
    portion = select_rows(blocks, places, per_device, capacity)
    cols = gather_tp(portion)
    down = swap(share(down_master, index, count, n).astype(BF))
    gate_serve = assemble(ring(gate, "grp"), index, count, per_device)
    up_serve = assemble(ring(up, "grp"), index, count, per_device)
    down_serve = assemble(ring(down, "grp"), index, count, per_device)
    hidden = first_matmuls(cols, gate_serve, up_serve, places)
    hidden = gather_tp(hidden)
    out = second_matmul(hidden, down_serve, places, lo, hi)
    out = swap(out)
    out = out.reshape(-1, out.shape[-1])
    mixed = combine(out, route_ids, route_weights, capacity)
    return (gate_serve, up_serve, down_serve, mixed)


def solution(mesh):
    grp, fs, tp = (mesh.shape["grp"], mesh.shape["fs"], mesh.shape["tp"])

    def build(*args):
        per_device = args[4].shape[0] // fs
        members = GROUP_SIZE // per_device
        split = Mesh(
            mesh.devices.reshape(grp, fs // members, members, tp // 2, 2),
            ("grp", "fh", "fl", "tp_0", "tp_1"),
        )
        in_specs = (
            P(("grp", *FS), None),
            P(("grp", *FS), None),
            P(("grp", *FS), None),
            P(FS),
            P(None, FS, TP),
            P(None, FS, TP),
            P(None, FS, TP),
        )
        out_specs = (
            P(("grp", *FS), None, TP),
            P(("grp", *FS), None, TP),
            P(("grp", *FS), None, TP),
            P(("grp", *FS), TP),
        )
        step = jax.shard_map(
            on_device, mesh=split, in_specs=in_specs, out_specs=out_specs, check_vma=False
        )
        return step(*args)

    return build
```

```python
import jax
import jax.numpy as jnp
from jax import lax
from jax.experimental import pallas as pl
from jax.experimental.pallas import tpu as pltpu
from jax.sharding import Mesh
from jax.sharding import PartitionSpec as P


GROUP_SIZE = 8
TP = ("tp_0", "tp_1")
BF = jnp.bfloat16
F32 = jnp.float32
LANES = 128

VM = pl.BlockSpec(memory_space=pltpu.VMEM)
ANY = pl.BlockSpec(memory_space=pl.ANY)


def shift(x, axis, k):
    n = lax.axis_size(axis)
    return lax.ppermute(x, axis, [(i, (i + k) % n) for i in range(n)])


def shape(dims, dtype=BF):
    return jax.ShapeDtypeStruct(dims, dtype)


def iota(dims, dim):
    return lax.broadcasted_iota(jnp.int32, dims, dim)


def dot(a, b, dims=((1,), (0,))):
    return lax.dot_general(a, b, (dims, ((), ())), preferred_element_type=F32)


def as_column(row):
    n = row.shape[1]
    same = iota((n, n), 0) == iota((n, n), 1)
    return jnp.sum(jnp.where(same, row, jnp.zeros_like(row)), axis=1, keepdims=True)


def slot_of(ids_ref, capacity):
    rows = ids_ref.shape[1]
    ids = [as_column(ids_ref[r : r + 1, :].astype(F32)) for r in range(2)]
    lane = iota((rows, LANES), 1).astype(F32)
    hits = [lane == i for i in ids]
    before = (iota((rows, rows), 0) > iota((rows, rows), 1)).astype(BF)
    count = dot(before, jnp.where(hits[0] | hits[1], 1.0, 0.0).astype(BF))
    return [
        (i * capacity + jnp.sum(jnp.where(h, count, 0.0), axis=1, keepdims=True)).astype(jnp.int32)
        for i, h in zip(ids, hits)
    ]


def pack_first(tokens, route_ids, gain, gate, n, count, capacity):
    tokens_n, model = tokens.shape
    _, whole, cols = gate.shape
    size = whole // count
    width = model // lax.axis_size(TP)
    slots = n * (whole // gain.shape[1]) * capacity
    each = slots // n
    pieces = width // LANES
    gain_rows = gain.shape[1]

    def body(tok_ref, ids_ref, gain_ref, gate_ref, out_ref, buf_ref, sem):
        start = pl.multiple_of(lax.axis_index("grp") * size, size)
        copy = pltpu.make_async_copy(gate_ref.at[:, pl.ds(start, size), :], buf_ref, sem)
        copy.start()
        tok = tok_ref[...].astype(F32)
        scale = lax.rsqrt(jnp.mean(tok * tok, axis=1, keepdims=True) + 1e-06)
        at = pl.multiple_of(lax.axis_index(TP) * width, width)
        own = (tok_ref[:, pl.ds(at, width)].astype(F32) * scale).astype(BF)
        first, second = slot_of(ids_ref, capacity)
        lane = iota((tokens_n, slots), 1)
        pick = jnp.where((lane == first) | (lane == second), 1.0, 0.0).astype(BF)
        filled = dot(pick, own, ((0,), (0,))).astype(BF)
        for j in range(n):
            for p in range(pieces):
                to = size + p * each
                out_ref[j, to : to + each, :] = filled[j * each : (j + 1) * each, p * LANES : (p + 1) * LANES]
        column = as_column(gain_ref[...])
        if size >= gain_rows:
            column = jnp.concatenate([column] * (size // gain_rows), axis=0)
        else:
            skip = lax.axis_index("grp") * size % gain_rows
            row = iota((size, gain_rows), 1) == iota((size, gain_rows), 0) + skip
            column = jnp.sum(jnp.where(row, gain_ref[...], 0.0), axis=1, keepdims=True)
        copy.wait()
        for j in range(n):
            out_ref[j, :size, :] = (buf_ref[j] * column).astype(BF)

    return pl.pallas_call(
        body,
        out_shape=shape((n, size + pieces * each, cols)),
        in_specs=[VM, VM, VM, ANY],
        out_specs=VM,
        scratch_shapes=[pltpu.VMEM((n, size, cols), F32), pltpu.SemaphoreType.DMA],
    )(tokens, route_ids.T, gain, gate)


def gather_tp(x):
    half = x.shape[0] // 2
    left, right = (shift(x, "tp_0", 1), shift(x, "tp_0", -1))
    across = (shift(left[:half], "tp_0", 1), shift(right[half:], "tp_0", -1))
    mine = (x, left, right, *across)
    return mine + tuple(shift(b, "tp_1", 1) for b in mine)


def pieces_of(refs):
    own, x = (lax.axis_index("tp_1"), lax.axis_index("tp_0"))
    for c in range(2):
        core = own if c == 0 else 1 - own
        for at, back in ((0, 0), (1, 3), (2, 1), (3, 2), (4, 2)):
            yield refs[5 * c + at], ((x + back) % 4) * 2 + core, at - 3 if at >= 3 else None


def span(part, rows):
    return slice(0, rows) if part is None else slice(part * rows // 2, (part + 1) * rows // 2)


def first_matmuls(blocks, gate, up, per_device, capacity):
    n, tall, _ = blocks[0].shape
    each = per_device * capacity
    pieces = tall // each
    cols = gate.shape[2]
    rows = n * capacity

    def body(*refs):
        ins, (gate_ref, up_ref, out_ref, acc_ref) = (refs[:10], refs[10:])
        for e in range(per_device):
            acc_ref[...] = jnp.zeros((rows, 2 * cols), F32)
            for ref, tp, part in pieces_of(ins):
                d = pl.ds(pl.multiple_of(tp * (pieces * LANES), pieces * LANES), pieces * LANES)
                w = jnp.concatenate([gate_ref[e, d, :], up_ref[e, d, :]], axis=1)
                x = [
                    ref[:, p * each + e * capacity : p * each + (e + 1) * capacity, :].reshape(-1, LANES)
                    for p in range(pieces)
                ]
                acc_ref[span(part, rows), :] += dot(jnp.concatenate(x, axis=1), w)
            g = acc_ref[:, :cols]
            out_ref[:, e * cols : (e + 1) * cols] = (g / (1.0 + jnp.exp(-g)) * acc_ref[:, cols:]).astype(BF)

    return pl.pallas_call(
        body,
        out_shape=shape((rows, per_device * cols)),
        in_specs=[VM] * 12,
        out_specs=VM,
        scratch_shapes=[pltpu.VMEM((rows, 2 * cols), F32)],
    )(*blocks, gate, up)


def second_matmul(blocks, down, n):
    rows = blocks[0].shape[0]
    per_device, _, cols = down.shape
    width = blocks[0].shape[1] // per_device
    capacity = rows // n

    def body(*refs):
        ins, (down_ref, out_ref, acc_ref) = (refs[:10], refs[10:])
        for e in range(per_device):
            acc_ref[...] = jnp.zeros((rows, cols), F32)
            for ref, tp, part in pieces_of(ins):
                w = down_ref[e, pl.ds(pl.multiple_of(tp * width, width), width), :]
                acc_ref[span(part, rows), :] += dot(ref[:, e * width : (e + 1) * width], w)
            out_ref[:, e] = acc_ref[...].reshape(n, capacity, cols).astype(BF)

    return pl.pallas_call(
        body,
        out_shape=shape((n, per_device, capacity, cols)),
        in_specs=[VM] * 11,
        out_specs=VM,
        scratch_shapes=[pltpu.VMEM((rows, cols), F32)],
    )(*blocks, down)


def combine(returned, route_ids, route_weights, capacity):
    rows, cols = (route_ids.shape[0], returned.shape[1])
    slots = returned.shape[0]

    def body(ret_ref, ids_ref, w_ref, out_ref):
        total = jnp.zeros((rows, cols), F32)
        for r, slot in enumerate(slot_of(ids_ref, capacity)):
            pick = (iota((rows, slots), 1) == slot).astype(BF)
            total = total + dot(pick, ret_ref[...]) * as_column(w_ref[r : r + 1, :])
        out_ref[...] = total.astype(BF)

    return pl.pallas_call(
        body, out_shape=shape((rows, cols)), in_specs=[VM] * 3, out_specs=VM
    )(returned, route_ids.T, route_weights.T)


def by_target(master, n):
    return master.reshape(n, -1, master.shape[2])


def share(master, index, count, n):
    whole = by_target(master, n)
    size = whole.shape[1] // count
    return lax.dynamic_slice_in_dim(whole, index * size, size, 1)


def ring(x, axis):
    n = lax.axis_size(axis)
    out, ahead, behind = ([(0, x)], x, x)
    for k in range(1, n // 2 + 1):
        ahead = shift(ahead, axis, 1)
        out.append((k, ahead))
        if k <= (n - 1) // 2:
            behind = shift(behind, axis, -1)
            out.append((n - k, behind))
    return out


def assemble(pieces, index, count, per_device):
    n, rows, cols = pieces[0][1].shape
    buffer = jnp.zeros((count, n, rows, cols), BF)
    for back, piece in pieces:
        at = (index - back) % count
        buffer = lax.dynamic_update_slice(buffer, piece[None], (at, 0, 0, 0))
    split = count // per_device
    buffer = buffer.reshape(per_device, split, n, rows, cols).transpose(0, 2, 1, 3, 4)
    return buffer.reshape(per_device, -1, cols)


def on_device(tokens, route_ids, route_weights, ffn_gain, gate_master, up_master, down_master):
    n = lax.axis_size("fs")
    count, index = (lax.axis_size("grp"), lax.axis_index("grp"))
    experts, rows, _ = gate_master.shape
    per_device = experts // n
    capacity = tokens.shape[0] // (2 * (experts // GROUP_SIZE))
    size = per_device * rows // count

    def swap(x):
        return lax.all_to_all(x, "fs", split_axis=0, concat_axis=0, tiled=True)

    packed = pack_first(
        tokens, route_ids, ffn_gain[None, :], by_target(gate_master, n), n, count, capacity
    )
    packed = swap(packed)
    if size < rows:
        gain = lax.dynamic_slice_in_dim(ffn_gain, index * size % rows, size)
    else:
        gain = jnp.concatenate([ffn_gain] * (size // rows))
    up = swap((share(up_master, index, count, n) * gain[None, :, None]).astype(BF))
    blocks = gather_tp(packed[:, size:])
    down = swap(share(down_master, index, count, n).astype(BF))
    gate_serve = assemble(ring(packed[:, :size], "grp"), index, count, per_device)
    up_serve = assemble(ring(up, "grp"), index, count, per_device)
    down_serve = assemble(ring(down, "grp"), index, count, per_device)
    hidden = first_matmuls(blocks, gate_serve, up_serve, per_device, capacity)
    hidden = gather_tp(hidden)
    out = second_matmul(hidden, down_serve, n)
    out = swap(out)
    mixed = combine(out.reshape(-1, out.shape[-1]), route_ids, route_weights, capacity)
    return (gate_serve, up_serve, down_serve, mixed)


def solution(mesh):
    grp, fs, tp = (mesh.shape["grp"], mesh.shape["fs"], mesh.shape["tp"])
    split = Mesh(mesh.devices.reshape(grp, fs, tp // 2, 2), ("grp", "fs", *TP))
    in_specs = (
        P(("grp", "fs"), None),
        P(("grp", "fs"), None),
        P(("grp", "fs"), None),
        P("fs"),
        P(None, "fs", TP),
        P(None, "fs", TP),
        P(None, "fs", TP),
    )
    out_specs = (
        P(("grp", "fs"), None, TP),
        P(("grp", "fs"), None, TP),
        P(("grp", "fs"), None, TP),
        P(("grp", "fs"), TP),
    )
    return jax.shard_map(on_device, mesh=split, in_specs=in_specs, out_specs=out_specs, check_vma=False)
```

```python
import jax
import jax.numpy as jnp
from jax import lax
from jax.experimental import pallas as pl
from jax.experimental.pallas import tpu as pltpu
from jax.sharding import Mesh
from jax.sharding import PartitionSpec as P


GROUP_SIZE = 8
TP = ("tp_0", "tp_1")
BF = jnp.bfloat16
F32 = jnp.float32
LANES = 128
META = 8

VM = pl.BlockSpec(memory_space=pltpu.VMEM)
ANY = pl.BlockSpec(memory_space=pl.ANY)


def shift(x, axis, k):
    n = lax.axis_size(axis)
    return lax.ppermute(x, axis, [(i, (i + k) % n) for i in range(n)])


def shape(dims, dtype=BF):
    return jax.ShapeDtypeStruct(dims, dtype)


def iota(dims, dim):
    return lax.broadcasted_iota(jnp.int32, dims, dim)


def dot(a, b, dims=((1,), (0,))):
    return lax.dot_general(a, b, (dims, ((), ())), preferred_element_type=F32)


def as_column(row):
    n = row.shape[1]
    same = iota((n, n), 0) == iota((n, n), 1)
    return jnp.sum(jnp.where(same, row, jnp.zeros_like(row)), axis=1, keepdims=True)


def slot_of(ids_ref, capacity):
    rows = ids_ref.shape[1]
    ids = [as_column(ids_ref[r : r + 1, :].astype(F32)) for r in range(2)]
    lane = iota((rows, LANES), 1).astype(F32)
    hits = [lane == i for i in ids]
    before = (iota((rows, rows), 0) > iota((rows, rows), 1)).astype(BF)
    count = dot(before, jnp.where(hits[0] | hits[1], 1.0, 0.0).astype(BF))
    return [
        (i * capacity + jnp.sum(jnp.where(h, count, 0.0), axis=1, keepdims=True)).astype(jnp.int32)
        for i, h in zip(ids, hits)
    ]


def fetch(pairs, sems):
    copies = [pltpu.make_async_copy(src, dst, sems.at[i]) for i, (src, dst) in enumerate(pairs)]
    for c in copies:
        c.start()
    return [c.wait for c in copies]


def pack_first(tokens, route_ids, gain, gate, n, count, groups):
    tokens_n, model = tokens.shape
    _, whole, cols = gate.shape
    size = whole // count
    width = model // lax.axis_size(TP)
    part = tokens_n // groups
    members = n // groups
    each = part // members
    pieces = width // LANES
    gain_rows = gain.shape[1]

    def body(tok_ref, ids_ref, gain_ref, gate_ref, out_ref, buf_ref, sem):
        start = pl.multiple_of(lax.axis_index("grp") * size, size)
        copy = pltpu.make_async_copy(gate_ref.at[:, pl.ds(start, size), :], buf_ref, sem)
        copy.start()
        tok = tok_ref[...].astype(F32)
        scale = lax.rsqrt(jnp.mean(tok * tok, axis=1, keepdims=True) + 1e-06)
        at = pl.multiple_of(lax.axis_index(TP) * width, width)
        own = (tok_ref[:, pl.ds(at, width)].astype(F32) * scale).astype(BF)
        ids = [as_column(ids_ref[r : r + 1, :].astype(F32)) for r in range(2)]
        group = ids[0].astype(jnp.int32) // GROUP_SIZE
        member = iota((tokens_n, LANES), 1) == group
        before = (iota((tokens_n, tokens_n), 0) > iota((tokens_n, tokens_n), 1)).astype(BF)
        count_before = dot(before, jnp.where(member, 1.0, 0.0).astype(BF))
        rank = jnp.sum(jnp.where(member, count_before, 0.0), axis=1, keepdims=True)
        place = iota((tokens_n, tokens_n), 1) == group * part + rank.astype(jnp.int32)
        ordered = dot(jnp.where(place, 1.0, 0.0).astype(BF), own, ((0,), (0,))).astype(BF)
        local = [i - (group * GROUP_SIZE).astype(F32) for i in ids]
        named = [jnp.sum(jnp.where(place, i, 0.0), axis=0, keepdims=True) for i in local]
        named = jnp.concatenate(named + [jnp.zeros((META - 2, tokens_n), F32)], axis=0)
        for j in range(n):
            first = j * each
            for p in range(pieces):
                to = size + p * each
                out_ref[j, to : to + each, :] = ordered[first : first + each, p * LANES : (p + 1) * LANES]
            a = j // members
            piece = named[:, a * part : (a + 1) * part]
            piece = jnp.concatenate([piece, jnp.zeros((META, LANES - part), F32)], axis=1)
            out_ref[j, size + pieces * each :, :] = piece.astype(BF)
        column = as_column(gain_ref[...])
        if size >= gain_rows:
            column = jnp.concatenate([column] * (size // gain_rows), axis=0)
        else:
            skip = lax.axis_index("grp") * size % gain_rows
            row = iota((size, gain_rows), 1) == iota((size, gain_rows), 0) + skip
            column = jnp.sum(jnp.where(row, gain_ref[...], 0.0), axis=1, keepdims=True)
        copy.wait()
        for j in range(n):
            out_ref[j, :size, :] = (buf_ref[j] * column).astype(BF)

    return pl.pallas_call(
        body,
        out_shape=shape((n, size + pieces * each + META, cols)),
        in_specs=[VM, VM, VM, ANY],
        out_specs=VM,
        scratch_shapes=[pltpu.VMEM((n, size, cols), F32), pltpu.SemaphoreType.DMA],
    )(tokens, route_ids.T, gain, gate)


def select_rows(blocks, named, per_device, capacity):
    members = len(blocks)
    n, tall, _ = blocks[0].shape
    pieces = 2 * LANES // LANES
    each = tall // pieces
    part = members * each

    def body(*refs):
        ins, (named_ref, *outs) = (refs[:members], refs[members : members + 1 + per_device])
        row_ref = refs[-1]
        here = lax.axis_index("fs") % members
        for k in range(members):
            back = here - k
            back = jnp.where(back < 0, back + members, back)
            to = pl.ds(pl.multiple_of(back * each, each), each)
            for p in range(pieces):
                row_ref[:, to, p * LANES : (p + 1) * LANES] = ins[k][:, p * each : (p + 1) * each, :]
        named_rows = named_ref[...].astype(F32)
        one, two = [
            jnp.concatenate([named_rows[j, r : r + 1, :part] for j in range(n)], axis=0) for r in range(2)
        ]
        earlier = (iota((part, part), 0) < iota((part, part), 1)).astype(BF)
        slot = iota((capacity, part), 0).astype(F32)
        ranks = []
        for k in range(per_device):
            e = here * per_device + expert_at(k, per_device)
            hit = (one == e.astype(F32)) | (two == e.astype(F32))
            rank = dot(jnp.where(hit, 1.0, 0.0).astype(BF), earlier)
            ranks.append(jnp.where(hit, rank, -1.0))
        for j in range(n):
            pick = [jnp.where(slot == ranks[k][j : j + 1], 1.0, 0.0) for k in range(per_device)]
            got = dot(jnp.concatenate(pick, axis=0).astype(BF), row_ref[j]).astype(BF)
            for k in range(per_device):
                for p in range(pieces):
                    outs[k][j, p * capacity : (p + 1) * capacity, :] = got[
                        k * capacity : (k + 1) * capacity, p * LANES : (p + 1) * LANES
                    ]

    return pl.pallas_call(
        body,
        out_shape=tuple(shape((n, pieces * capacity, LANES)) for _ in range(per_device)),
        in_specs=[VM] * (members + 1),
        out_specs=tuple(VM for _ in range(per_device)),
        scratch_shapes=[pltpu.VMEM((n, part, pieces * LANES), BF)],
    )(*blocks, named)


def expert_at(k, per_device):
    return (lax.axis_index("grp") + per_device - k) % per_device


def gather_tp(x, back):
    left, right = (shift(x, "tp_0", 1), shift(x, "tp_0", -1))
    across = shift(right, "tp_0", -1) if back else shift(left, "tp_0", 1)
    mine = (x, left, right, across)
    return mine + tuple(shift(b, "tp_1", 1) for b in mine)


def places_of():
    own, x = (lax.axis_index("tp_1"), lax.axis_index("tp_0"))
    return [
        ((x + ahead) % 4) * 2 + core for core in (own, 1 - own) for ahead in (0, 3, 1, 2)
    ]


def first_matmuls(blocks, gate, up, capacity):
    n, tall, _ = blocks[0].shape
    pieces = tall // capacity
    depth, cols = gate.shape
    rows = n * capacity
    count = len(blocks)

    def body(*refs):
        ins, (gate_ref, up_ref, out_ref, in_buf, gate_buf, up_buf, acc_ref, sems) = (
            refs[:count],
            refs[count:],
        )
        waits = fetch(
            [(gate_ref, gate_buf), (up_ref, up_buf)] + [(r, in_buf.at[i]) for i, r in enumerate(ins)], sems
        )
        waits[0]()
        waits[1]()
        for i, tp in enumerate(places_of()):
            d = pl.ds(pl.multiple_of(tp * (pieces * LANES), pieces * LANES), pieces * LANES)
            w = jnp.concatenate([gate_buf[d, :], up_buf[d, :]], axis=1)
            waits[2 + i]()
            x = [
                in_buf[i, :, p * capacity : (p + 1) * capacity, :].reshape(rows, LANES)
                for p in range(pieces)
            ]
            more = dot(jnp.concatenate(x, axis=1), w)
            if i == 0:
                acc_ref[...] = more
            else:
                acc_ref[...] += more
        g = acc_ref[:, :cols]
        out_ref[...] = (g / (1.0 + jnp.exp(-g)) * acc_ref[:, cols:]).astype(BF)

    return pl.pallas_call(
        body,
        out_shape=shape((rows, cols)),
        in_specs=[ANY] * (count + 2),
        out_specs=VM,
        scratch_shapes=[
            pltpu.VMEM((count, n, tall, LANES), BF),
            pltpu.VMEM((depth, cols), BF),
            pltpu.VMEM((depth, cols), BF),
            pltpu.VMEM((rows, 2 * cols), F32),
            pltpu.SemaphoreType.DMA((count + 2,)),
        ],
    )(*blocks, gate, up)


def second_matmul(blocks, down, n, k, per_device, before):
    rows, width = blocks[0].shape
    depth, cols = down.shape
    capacity = rows // n
    count = len(blocks)
    given = 0 if before is None else 1

    def body(*refs):
        ins, rest = (refs[:count], refs[count : count + 1] + refs[count + 1 + given :])
        down_ref, out_ref, in_buf, down_buf, acc_ref, row_ref, sems, sem = rest
        waits = fetch([(down_ref, down_buf)] + [(r, in_buf.at[i]) for i, r in enumerate(ins)], sems)
        waits[0]()
        for i, tp in enumerate(places_of()):
            w = down_buf[pl.ds(pl.multiple_of(tp * width, width), width), :]
            waits[1 + i]()
            more = dot(in_buf[i], w)
            if i == 0:
                acc_ref[...] = more
            else:
                acc_ref[...] += more
        row_ref[...] = acc_ref[...].reshape(n, capacity, cols).astype(BF)
        copy = pltpu.make_async_copy(row_ref, out_ref.at[:, expert_at(k, per_device)], sem)
        copy.start()
        copy.wait()

    return pl.pallas_call(
        body,
        out_shape=shape((n, per_device, capacity, cols)),
        in_specs=[ANY] * (count + 1 + given),
        out_specs=ANY,
        input_output_aliases={count + 1: 0} if given else {},
        scratch_shapes=[
            pltpu.VMEM((count, rows, width), BF),
            pltpu.VMEM((depth, cols), BF),
            pltpu.VMEM((rows, cols), F32),
            pltpu.VMEM((n, capacity, cols), BF),
            pltpu.SemaphoreType.DMA((count + 1,)),
            pltpu.SemaphoreType.DMA,
        ],
    )(*blocks, down, *([] if before is None else [before]))


def combine(returned, route_ids, route_weights, capacity):
    rows, cols = (route_ids.shape[0], returned.shape[1])
    slots = returned.shape[0]

    def body(ret_ref, ids_ref, w_ref, out_ref):
        total = jnp.zeros((rows, cols), F32)
        for r, slot in enumerate(slot_of(ids_ref, capacity)):
            pick = (iota((rows, slots), 1) == slot).astype(BF)
            total = total + dot(pick, ret_ref[...]) * as_column(w_ref[r : r + 1, :])
        out_ref[...] = total.astype(BF)

    return pl.pallas_call(
        body, out_shape=shape((rows, cols)), in_specs=[VM] * 3, out_specs=VM
    )(returned, route_ids.T, route_weights.T)


def by_target(master, n):
    return master.reshape(n, -1, master.shape[2])


def share(master, index, count, n):
    whole = by_target(master, n)
    size = whole.shape[1] // count
    return lax.dynamic_slice_in_dim(whole, index * size, size, 1)


def ring(x, axis):
    n = lax.axis_size(axis)
    out, ahead, behind = ([(0, x)], x, x)
    for k in range(1, n // 2 + 1):
        ahead = shift(ahead, axis, 1)
        out.append((k, ahead))
        if k <= (n - 1) // 2:
            behind = shift(behind, axis, -1)
            out.append((n - k, behind))
    return out


def assemble(pieces, index, count, per_device):
    n, rows, cols = pieces[0][1].shape
    buffer = jnp.zeros((count, n, rows, cols), BF)
    for back, piece in pieces:
        at = (index - back) % count
        buffer = lax.dynamic_update_slice(buffer, piece[None], (at, 0, 0, 0))
    split = count // per_device
    buffer = buffer.reshape(per_device, split, n, rows, cols).transpose(0, 2, 1, 3, 4)
    return buffer.reshape(per_device, -1, cols)


def one_by_one(pieces, served, index, count, per_device):
    if count == per_device:
        return [p.reshape(-1, p.shape[-1]) for _, p in sorted(pieces, key=lambda q: q[0])]
    return [
        lax.dynamic_index_in_dim(served, (index + per_device - k) % per_device, 0, False)
        for k in range(per_device)
    ]


def on_device(tokens, route_ids, route_weights, ffn_gain, gate_master, up_master, down_master):
    n = lax.axis_size("fs")
    count, index = (lax.axis_size("grp"), lax.axis_index("grp"))
    experts, rows, _ = gate_master.shape
    per_device = experts // n
    groups = experts // GROUP_SIZE
    members = n // groups
    capacity = tokens.shape[0] // (2 * groups)
    size = per_device * rows // count

    def swap(x):
        return lax.all_to_all(x, "fs", split_axis=0, concat_axis=0, tiled=True)

    def neighbour(x, k):
        pairs = [(i, i - i % members + (i + k) % members) for i in range(n)]
        return lax.ppermute(x, "fs", pairs)

    packed = pack_first(
        tokens, route_ids, ffn_gain[None, :], by_target(gate_master, n), n, count, groups
    )
    packed = swap(packed)
    gate, near, named = jnp.split(packed, [size, packed.shape[1] - META], axis=1)
    near = [near] + [neighbour(near, k) for k in range(1, members)]
    if size < rows:
        gain = lax.dynamic_slice_in_dim(ffn_gain, index * size % rows, size)
    else:
        gain = jnp.concatenate([ffn_gain] * (size // rows))
    up = swap((share(up_master, index, count, n) * gain[None, :, None]).astype(BF))
    chosen = select_rows(near, named, per_device, capacity)
    down = swap(share(down_master, index, count, n).astype(BF))
    gate = ring(gate, "grp")
    up = ring(up, "grp")
    down = ring(down, "grp")
    gate_serve = assemble(gate, index, count, per_device)
    up_serve = assemble(up, index, count, per_device)
    down_serve = assemble(down, index, count, per_device)
    gates = one_by_one(gate, gate_serve, index, count, per_device)
    ups = one_by_one(up, up_serve, index, count, per_device)
    downs = one_by_one(down, down_serve, index, count, per_device)
    out = None
    for k in range(per_device):
        blocks = gather_tp(chosen[k], k % 2)
        hidden = first_matmuls(blocks, gates[k], ups[k], capacity)
        hidden = gather_tp(hidden, k % 2)
        out = second_matmul(hidden, downs[k], n, k, per_device, out)
    out = swap(out)
    mixed = combine(out.reshape(-1, out.shape[-1]), route_ids, route_weights, capacity)
    return (gate_serve, up_serve, down_serve, mixed)


def solution(mesh):
    grp, fs, tp = (mesh.shape["grp"], mesh.shape["fs"], mesh.shape["tp"])
    split = Mesh(mesh.devices.reshape(grp, fs, tp // 2, 2), ("grp", "fs", *TP))
    in_specs = (
        P(("grp", "fs"), None),
        P(("grp", "fs"), None),
        P(("grp", "fs"), None),
        P("fs"),
        P(None, "fs", TP),
        P(None, "fs", TP),
        P(None, "fs", TP),
    )
    out_specs = (
        P(("grp", "fs"), None, TP),
        P(("grp", "fs"), None, TP),
        P(("grp", "fs"), None, TP),
        P(("grp", "fs"), TP),
    )
    return jax.shard_map(
        on_device, mesh=split, in_specs=in_specs, out_specs=out_specs, check_vma=False
    )
```

```python
import jax
import jax.numpy as jnp
from jax import lax
from jax.experimental import pallas as pl
from jax.experimental.pallas import tpu as pltpu
from jax.sharding import Mesh
from jax.sharding import PartitionSpec as P


GROUP_SIZE = 8
TP = ("tp_0", "tp_1")
BF = jnp.bfloat16
F32 = jnp.float32
LANES = 128
META = 8

VM = pl.BlockSpec(memory_space=pltpu.VMEM)
ANY = pl.BlockSpec(memory_space=pl.ANY)


def shift(x, axis, k):
    n = lax.axis_size(axis)
    return lax.ppermute(x, axis, [(i, (i + k) % n) for i in range(n)])


def shape(dims, dtype=BF):
    return jax.ShapeDtypeStruct(dims, dtype)


def iota(dims, dim):
    return lax.broadcasted_iota(jnp.int32, dims, dim)


def dot(a, b, dims=((1,), (0,))):
    return lax.dot_general(a, b, (dims, ((), ())), preferred_element_type=F32)


def as_column(row):
    n = row.shape[1]
    same = iota((n, n), 0) == iota((n, n), 1)
    return jnp.sum(jnp.where(same, row, jnp.zeros_like(row)), axis=1, keepdims=True)


def slot_of(ids_ref, capacity):
    rows = ids_ref.shape[1]
    ids = [as_column(ids_ref[r : r + 1, :].astype(F32)) for r in range(2)]
    lane = iota((rows, LANES), 1).astype(F32)
    hits = [lane == i for i in ids]
    before = (iota((rows, rows), 0) > iota((rows, rows), 1)).astype(BF)
    count = dot(before, jnp.where(hits[0] | hits[1], 1.0, 0.0).astype(BF))
    return [
        (i * capacity + jnp.sum(jnp.where(h, count, 0.0), axis=1, keepdims=True)).astype(jnp.int32)
        for i, h in zip(ids, hits)
    ]


def fetch(pairs, sems):
    copies = [pltpu.make_async_copy(src, dst, sems.at[i]) for i, (src, dst) in enumerate(pairs)]
    for c in copies:
        c.start()
    return [c.wait for c in copies]


def pack_first(tokens, route_ids, gain, gate, n, count, groups):
    tokens_n, model = tokens.shape
    _, whole, cols = gate.shape
    size = whole // count
    width = model // lax.axis_size(TP)
    part = tokens_n // groups
    members = n // groups
    each = part // members
    pieces = width // LANES
    gain_rows = gain.shape[1]

    def body(tok_ref, ids_ref, gain_ref, gate_ref, out_ref, buf_ref, sem):
        start = pl.multiple_of(lax.axis_index("grp") * size, size)
        copy = pltpu.make_async_copy(gate_ref.at[:, pl.ds(start, size), :], buf_ref, sem)
        copy.start()
        tok = tok_ref[...].astype(F32)
        scale = lax.rsqrt(jnp.mean(tok * tok, axis=1, keepdims=True) + 1e-06)
        at = pl.multiple_of(lax.axis_index(TP) * width, width)
        own = (tok_ref[:, pl.ds(at, width)].astype(F32) * scale).astype(BF)
        ids = [as_column(ids_ref[r : r + 1, :].astype(F32)) for r in range(2)]
        group = ids[0].astype(jnp.int32) // GROUP_SIZE
        member = iota((tokens_n, LANES), 1) == group
        before = (iota((tokens_n, tokens_n), 0) > iota((tokens_n, tokens_n), 1)).astype(BF)
        count_before = dot(before, jnp.where(member, 1.0, 0.0).astype(BF))
        rank = jnp.sum(jnp.where(member, count_before, 0.0), axis=1, keepdims=True)
        place = iota((tokens_n, tokens_n), 1) == group * part + rank.astype(jnp.int32)
        ordered = dot(jnp.where(place, 1.0, 0.0).astype(BF), own, ((0,), (0,))).astype(BF)
        local = [i - (group * GROUP_SIZE).astype(F32) for i in ids]
        named = [jnp.sum(jnp.where(place, i, 0.0), axis=0, keepdims=True) for i in local]
        named = jnp.concatenate(named + [jnp.zeros((META - 2, tokens_n), F32)], axis=0)
        for j in range(n):
            first = j * each
            for p in range(pieces):
                to = size + p * each
                out_ref[j, to : to + each, :] = ordered[first : first + each, p * LANES : (p + 1) * LANES]
            a = j // members
            piece = named[:, a * part : (a + 1) * part]
            piece = jnp.concatenate([piece, jnp.zeros((META, LANES - part), F32)], axis=1)
            out_ref[j, size + pieces * each :, :] = piece.astype(BF)
        column = as_column(gain_ref[...])
        if size >= gain_rows:
            column = jnp.concatenate([column] * (size // gain_rows), axis=0)
        else:
            skip = lax.axis_index("grp") * size % gain_rows
            row = iota((size, gain_rows), 1) == iota((size, gain_rows), 0) + skip
            column = jnp.sum(jnp.where(row, gain_ref[...], 0.0), axis=1, keepdims=True)
        copy.wait()
        for j in range(n):
            out_ref[j, :size, :] = (buf_ref[j] * column).astype(BF)

    return pl.pallas_call(
        body,
        out_shape=shape((n, size + pieces * each + META, cols)),
        in_specs=[VM, VM, VM, ANY],
        out_specs=VM,
        scratch_shapes=[pltpu.VMEM((n, size, cols), F32), pltpu.SemaphoreType.DMA],
    )(tokens, route_ids.T, gain, gate)


def select_rows(blocks, named, per_device, capacity):
    members = len(blocks)
    n, tall, _ = blocks[0].shape
    pieces = 2 * LANES // LANES
    each = tall // pieces
    part = members * each

    def body(*refs):
        ins, (named_ref, *outs) = (refs[:members], refs[members : members + 1 + per_device])
        row_ref = refs[-1]
        here = lax.axis_index("fs") % members
        for k in range(members):
            back = here - k
            back = jnp.where(back < 0, back + members, back)
            to = pl.ds(pl.multiple_of(back * each, each), each)
            for p in range(pieces):
                row_ref[:, to, p * LANES : (p + 1) * LANES] = ins[k][:, p * each : (p + 1) * each, :]
        named_rows = named_ref[...].astype(F32)
        one, two = [
            jnp.concatenate([named_rows[j, r : r + 1, :part] for j in range(n)], axis=0) for r in range(2)
        ]
        earlier = (iota((part, part), 0) < iota((part, part), 1)).astype(BF)
        slot = iota((capacity, part), 0).astype(F32)
        ranks = []
        for k in range(per_device):
            e = here * per_device + expert_at(k, per_device)
            hit = (one == e.astype(F32)) | (two == e.astype(F32))
            rank = dot(jnp.where(hit, 1.0, 0.0).astype(BF), earlier)
            ranks.append(jnp.where(hit, rank, -1.0))
        for j in range(n):
            pick = [jnp.where(slot == ranks[k][j : j + 1], 1.0, 0.0) for k in range(per_device)]
            got = dot(jnp.concatenate(pick, axis=0).astype(BF), row_ref[j]).astype(BF)
            for k in range(per_device):
                for p in range(pieces):
                    outs[k][j, p * capacity : (p + 1) * capacity, :] = got[
                        k * capacity : (k + 1) * capacity, p * LANES : (p + 1) * LANES
                    ]

    return pl.pallas_call(
        body,
        out_shape=tuple(shape((n, pieces * capacity, LANES)) for _ in range(per_device)),
        in_specs=[VM] * (members + 1),
        out_specs=tuple(VM for _ in range(per_device)),
        scratch_shapes=[pltpu.VMEM((n, part, pieces * LANES), BF)],
    )(*blocks, named)


def expert_at(k, per_device):
    return (lax.axis_index("grp") + per_device - k) % per_device


def gather_tp(x, back):
    left, right = (shift(x, "tp_0", 1), shift(x, "tp_0", -1))
    across = shift(right, "tp_0", -1) if back else shift(left, "tp_0", 1)
    mine = (x, left, right, across)
    return mine + tuple(shift(b, "tp_1", 1) for b in mine)


def places_of():
    own, x = (lax.axis_index("tp_1"), lax.axis_index("tp_0"))
    return [
        ((x + ahead) % 4) * 2 + core for core in (own, 1 - own) for ahead in (0, 3, 1, 2)
    ]


def first_matmuls(blocks, gate, up, capacity):
    n, tall, _ = blocks[0].shape
    pieces = tall // capacity
    width = pieces * LANES
    depth, cols = gate.shape
    rows = n * capacity
    count = len(blocks)

    def body(*refs):
        ins, (gate_ref, up_ref, out_ref, in_buf, w_buf, sems) = (refs[:count], refs[count:])
        pairs = []
        for i, tp in enumerate(places_of()):
            d = pl.ds(pl.multiple_of(tp * width, width), width)
            to = slice(i * width, (i + 1) * width)
            pairs += [(gate_ref.at[d, :], w_buf.at[to, :cols]), (up_ref.at[d, :], w_buf.at[to, cols:])]
            for p in range(pieces):
                lanes = slice(i * width + p * LANES, i * width + (p + 1) * LANES)
                pairs.append(
                    (ins[i].at[:, p * capacity : (p + 1) * capacity, :], in_buf.at[:, :, lanes])
                )
        for wait in fetch(pairs, sems):
            wait()
        both = dot(in_buf[...].reshape(rows, depth), w_buf[...])
        g = both[:, :cols]
        out_ref[...] = (g / (1.0 + jnp.exp(-g)) * both[:, cols:]).astype(BF)

    return pl.pallas_call(
        body,
        out_shape=shape((rows, cols)),
        in_specs=[ANY] * (count + 2),
        out_specs=VM,
        scratch_shapes=[
            pltpu.VMEM((n, capacity, depth), BF),
            pltpu.VMEM((depth, 2 * cols), BF),
            pltpu.SemaphoreType.DMA((count * (2 + pieces),)),
        ],
    )(*blocks, gate, up)


def second_matmul(blocks, down, n):
    rows, width = blocks[0].shape
    depth, cols = down.shape
    capacity = rows // n
    count = len(blocks)

    def body(*refs):
        ins, (down_ref, out_ref, in_buf, down_buf, sems) = (refs[:count], refs[count:])
        pairs = []
        for i, tp in enumerate(places_of()):
            d = pl.ds(pl.multiple_of(tp * width, width), width)
            to = slice(i * width, (i + 1) * width)
            pairs += [(down_ref.at[d, :], down_buf.at[to, :]), (ins[i], in_buf.at[:, to])]
        for wait in fetch(pairs, sems):
            wait()
        out_ref[...] = dot(in_buf[...], down_buf[...]).reshape(n, capacity, cols).astype(BF)

    return pl.pallas_call(
        body,
        out_shape=shape((n, capacity, cols)),
        in_specs=[ANY] * (count + 1),
        out_specs=VM,
        scratch_shapes=[
            pltpu.VMEM((rows, depth), BF),
            pltpu.VMEM((depth, cols), BF),
            pltpu.SemaphoreType.DMA((2 * count,)),
        ],
    )(*blocks, down)


def combine(returned, route_ids, route_weights, capacity, k, per_device, so_far):
    rows, cols = (route_ids.shape[0], returned.shape[1])
    slots = returned.shape[0]
    last = k == per_device - 1

    def body(ret_ref, ids_ref, w_ref, *refs):
        out_ref = refs[-1]
        total = jnp.zeros((rows, cols), F32) if so_far is None else refs[0][...]
        for r, slot in enumerate(slot_of(ids_ref, capacity)):
            expert, at = (slot // capacity, slot % capacity)
            mine = expert % per_device == expert_at(k, per_device)
            to = jnp.where(mine, expert // per_device * capacity + at, -1)
            pick = jnp.where(iota((rows, slots), 1) == to, 1.0, 0.0).astype(BF)
            total = total + dot(pick, ret_ref[...]) * as_column(w_ref[r : r + 1, :])
        out_ref[...] = total.astype(out_ref.dtype)

    given = [] if so_far is None else [so_far]
    return pl.pallas_call(
        body,
        out_shape=shape((rows, cols), BF if last else F32),
        in_specs=[VM] * (3 + len(given)),
        out_specs=VM,
    )(returned, route_ids.T, route_weights.T, *given)


def by_target(master, n):
    return master.reshape(n, -1, master.shape[2])


def share(master, index, count, n):
    whole = by_target(master, n)
    size = whole.shape[1] // count
    return lax.dynamic_slice_in_dim(whole, index * size, size, 1)


def ring(x, axis):
    n = lax.axis_size(axis)
    out, ahead, behind = ([(0, x)], x, x)
    for k in range(1, n // 2 + 1):
        ahead = shift(ahead, axis, 1)
        out.append((k, ahead))
        if k <= (n - 1) // 2:
            behind = shift(behind, axis, -1)
            out.append((n - k, behind))
    return out


def assemble(pieces, index, count, per_device):
    n, rows, cols = pieces[0][1].shape
    buffer = jnp.zeros((count, n, rows, cols), BF)
    for back, piece in pieces:
        at = (index - back) % count
        buffer = lax.dynamic_update_slice(buffer, piece[None], (at, 0, 0, 0))
    split = count // per_device
    buffer = buffer.reshape(per_device, split, n, rows, cols).transpose(0, 2, 1, 3, 4)
    return buffer.reshape(per_device, -1, cols)


def one_by_one(pieces, served, index, count, per_device):
    if count == per_device:
        return [p.reshape(-1, p.shape[-1]) for _, p in sorted(pieces, key=lambda q: q[0])]
    return [
        lax.dynamic_index_in_dim(served, (index + per_device - k) % per_device, 0, False)
        for k in range(per_device)
    ]


def on_device(tokens, route_ids, route_weights, ffn_gain, gate_master, up_master, down_master):
    n = lax.axis_size("fs")
    count, index = (lax.axis_size("grp"), lax.axis_index("grp"))
    experts, rows, _ = gate_master.shape
    per_device = experts // n
    groups = experts // GROUP_SIZE
    members = n // groups
    capacity = tokens.shape[0] // (2 * groups)
    size = per_device * rows // count

    def swap(x):
        return lax.all_to_all(x, "fs", split_axis=0, concat_axis=0, tiled=True)

    def neighbour(x, k):
        pairs = [(i, i - i % members + (i + k) % members) for i in range(n)]
        return lax.ppermute(x, "fs", pairs)

    packed = pack_first(
        tokens, route_ids, ffn_gain[None, :], by_target(gate_master, n), n, count, groups
    )
    packed = swap(packed)
    gate, near, named = jnp.split(packed, [size, packed.shape[1] - META], axis=1)
    near = [near] + [neighbour(near, k) for k in range(1, members)]
    if size < rows:
        gain = lax.dynamic_slice_in_dim(ffn_gain, index * size % rows, size)
    else:
        gain = jnp.concatenate([ffn_gain] * (size // rows))
    up = swap((share(up_master, index, count, n) * gain[None, :, None]).astype(BF))
    chosen = select_rows(near, named, per_device, capacity)
    down = swap(share(down_master, index, count, n).astype(BF))
    gate = ring(gate, "grp")
    up = ring(up, "grp")
    down = ring(down, "grp")
    gate_serve = assemble(gate, index, count, per_device)
    up_serve = assemble(up, index, count, per_device)
    down_serve = assemble(down, index, count, per_device)
    gates = one_by_one(gate, gate_serve, index, count, per_device)
    ups = one_by_one(up, up_serve, index, count, per_device)
    downs = one_by_one(down, down_serve, index, count, per_device)
    mixed = None
    for k in range(per_device):
        blocks = gather_tp(chosen[k], k % 2)
        hidden = first_matmuls(blocks, gates[k], ups[k], capacity)
        hidden = gather_tp(hidden, k % 2)
        out = second_matmul(hidden, downs[k], n)
        out = swap(out).reshape(-1, out.shape[-1])
        mixed = combine(out, route_ids, route_weights, capacity, k, per_device, mixed)
    return (gate_serve, up_serve, down_serve, mixed)


def solution(mesh):
    grp, fs, tp = (mesh.shape["grp"], mesh.shape["fs"], mesh.shape["tp"])
    split = Mesh(mesh.devices.reshape(grp, fs, tp // 2, 2), ("grp", "fs", *TP))
    in_specs = (
        P(("grp", "fs"), None),
        P(("grp", "fs"), None),
        P(("grp", "fs"), None),
        P("fs"),
        P(None, "fs", TP),
        P(None, "fs", TP),
        P(None, "fs", TP),
    )
    out_specs = (
        P(("grp", "fs"), None, TP),
        P(("grp", "fs"), None, TP),
        P(("grp", "fs"), None, TP),
        P(("grp", "fs"), TP),
    )
    return jax.shard_map(on_device, mesh=split, in_specs=in_specs, out_specs=out_specs, check_vma=False)
```

```python
import jax
import jax.numpy as jnp
from jax import lax
from jax.experimental import pallas as pl
from jax.experimental.pallas import tpu as pltpu
from jax.sharding import Mesh
from jax.sharding import PartitionSpec as P


GROUP_SIZE = 8
TP = ("tp_0", "tp_1")
BF = jnp.bfloat16
F32 = jnp.float32
LANES = 128
META = 8
LIMIT = pltpu.CompilerParams(vmem_limit_bytes=14 * 2**20)

VM = pl.BlockSpec(memory_space=pltpu.VMEM)
ANY = pl.BlockSpec(memory_space=pl.ANY)


def shift(x, axis, k):
    n = lax.axis_size(axis)
    return lax.ppermute(x, axis, [(i, (i + k) % n) for i in range(n)])


def shape(dims, dtype=BF):
    return jax.ShapeDtypeStruct(dims, dtype)


def held(dims, dtype=BF):
    return pltpu.VMEM(dims, dtype)


def near_core(arrays):
    return [pltpu.with_memory_space_constraint(a, pltpu.VMEM) for a in arrays]


def iota(dims, dim):
    return lax.broadcasted_iota(jnp.int32, dims, dim)


def dot(a, b, dims=((1,), (0,))):
    return lax.dot_general(a, b, (dims, ((), ())), preferred_element_type=F32)


def as_column(row):
    n = row.shape[1]
    same = iota((n, n), 0) == iota((n, n), 1)
    return jnp.sum(jnp.where(same, row, jnp.zeros_like(row)), axis=1, keepdims=True)


def slot_of(ids_ref, capacity):
    rows = ids_ref.shape[1]
    ids = [as_column(ids_ref[r : r + 1, :].astype(F32)) for r in range(2)]
    lane = iota((rows, LANES), 1).astype(F32)
    hits = [lane == i for i in ids]
    before = (iota((rows, rows), 0) > iota((rows, rows), 1)).astype(BF)
    count = dot(before, jnp.where(hits[0] | hits[1], 1.0, 0.0).astype(BF))
    return [
        (i * capacity + jnp.sum(jnp.where(h, count, 0.0), axis=1, keepdims=True)).astype(jnp.int32)
        for i, h in zip(ids, hits)
    ]


def pack_first(tokens, route_ids, gain, gate, n, count, groups):
    tokens_n, model = tokens.shape
    _, whole, cols = gate.shape
    size = whole // count
    width = model // lax.axis_size(TP)
    part = tokens_n // groups
    members = n // groups
    each = part // members
    pieces = width // LANES
    gain_rows = gain.shape[1]

    def body(tok_ref, ids_ref, gain_ref, gate_ref, out_ref, buf_ref, sem):
        start = pl.multiple_of(lax.axis_index("grp") * size, size)
        copy = pltpu.make_async_copy(gate_ref.at[:, pl.ds(start, size), :], buf_ref, sem)
        copy.start()
        tok = tok_ref[...].astype(F32)
        scale = lax.rsqrt(jnp.mean(tok * tok, axis=1, keepdims=True) + 1e-06)
        at = pl.multiple_of(lax.axis_index(TP) * width, width)
        own = (tok_ref[:, pl.ds(at, width)].astype(F32) * scale).astype(BF)
        ids = [as_column(ids_ref[r : r + 1, :].astype(F32)) for r in range(2)]
        group = ids[0].astype(jnp.int32) // GROUP_SIZE
        member = iota((tokens_n, LANES), 1) == group
        before = (iota((tokens_n, tokens_n), 0) > iota((tokens_n, tokens_n), 1)).astype(BF)
        count_before = dot(before, jnp.where(member, 1.0, 0.0).astype(BF))
        rank = jnp.sum(jnp.where(member, count_before, 0.0), axis=1, keepdims=True)
        place = iota((tokens_n, tokens_n), 1) == group * part + rank.astype(jnp.int32)
        ordered = dot(jnp.where(place, 1.0, 0.0).astype(BF), own, ((0,), (0,))).astype(BF)
        local = [i - (group * GROUP_SIZE).astype(F32) for i in ids]
        named = [jnp.sum(jnp.where(place, i, 0.0), axis=0, keepdims=True) for i in local]
        named = jnp.concatenate(named + [jnp.zeros((META - 2, tokens_n), F32)], axis=0)
        for j in range(n):
            first = j * each
            for p in range(pieces):
                to = size + p * each
                out_ref[j, to : to + each, :] = ordered[first : first + each, p * LANES : (p + 1) * LANES]
            a = j // members
            piece = named[:, a * part : (a + 1) * part]
            piece = jnp.concatenate([piece, jnp.zeros((META, LANES - part), F32)], axis=1)
            out_ref[j, size + pieces * each :, :] = piece.astype(BF)
        column = as_column(gain_ref[...])
        if size >= gain_rows:
            column = jnp.concatenate([column] * (size // gain_rows), axis=0)
        else:
            skip = lax.axis_index("grp") * size % gain_rows
            row = iota((size, gain_rows), 1) == iota((size, gain_rows), 0) + skip
            column = jnp.sum(jnp.where(row, gain_ref[...], 0.0), axis=1, keepdims=True)
        copy.wait()
        for j in range(n):
            out_ref[j, :size, :] = (buf_ref[j] * column).astype(BF)

    return pl.pallas_call(
        body,
        out_shape=shape((n, size + pieces * each + META, cols)),
        in_specs=[VM, VM, VM, ANY],
        out_specs=VM,
        scratch_shapes=[pltpu.VMEM((n, size, cols), F32), pltpu.SemaphoreType.DMA],
    )(tokens, route_ids.T, gain, gate)


def select_rows(blocks, named, per_device, capacity):
    members = len(blocks)
    n, tall, _ = blocks[0].shape
    pieces = 2 * LANES // LANES
    each = tall // pieces
    part = members * each

    def body(*refs):
        ins, (named_ref, *outs) = (refs[:members], refs[members : members + 1 + per_device])
        row_ref = refs[-1]
        here = lax.axis_index("fs") % members
        for k in range(members):
            back = here - k
            back = jnp.where(back < 0, back + members, back)
            to = pl.ds(pl.multiple_of(back * each, each), each)
            for p in range(pieces):
                row_ref[:, to, p * LANES : (p + 1) * LANES] = ins[k][:, p * each : (p + 1) * each, :]
        named_rows = named_ref[...].astype(F32)
        one, two = [
            jnp.concatenate([named_rows[j, r : r + 1, :part] for j in range(n)], axis=0) for r in range(2)
        ]
        earlier = (iota((part, part), 0) < iota((part, part), 1)).astype(BF)
        slot = iota((capacity, part), 0).astype(F32)
        ranks = []
        for k in range(per_device):
            e = here * per_device + expert_at(k, per_device)
            hit = (one == e.astype(F32)) | (two == e.astype(F32))
            rank = dot(jnp.where(hit, 1.0, 0.0).astype(BF), earlier)
            ranks.append(jnp.where(hit, rank, -1.0))
        for j in range(n):
            pick = [jnp.where(slot == ranks[k][j : j + 1], 1.0, 0.0) for k in range(per_device)]
            got = dot(jnp.concatenate(pick, axis=0).astype(BF), row_ref[j]).astype(BF)
            for k in range(per_device):
                for p in range(pieces):
                    outs[k][j, p * capacity : (p + 1) * capacity, :] = got[
                        k * capacity : (k + 1) * capacity, p * LANES : (p + 1) * LANES
                    ]

    return pl.pallas_call(
        body,
        out_shape=tuple(held((n, pieces * capacity, LANES)) for _ in range(per_device)),
        in_specs=[VM] * (members + 1),
        out_specs=tuple(VM for _ in range(per_device)),
        compiler_params=LIMIT,
        scratch_shapes=[pltpu.VMEM((n, part, pieces * LANES), BF)],
    )(*near_core([*blocks, named]))


def expert_at(k, per_device):
    return (lax.axis_index("grp") + per_device - k) % per_device


def gather_tp(x, back):
    left, right = (shift(x, "tp_0", 1), shift(x, "tp_0", -1))
    across = shift(right, "tp_0", -1) if back else shift(left, "tp_0", 1)
    mine = (x, left, right, across)
    return mine + tuple(shift(b, "tp_1", 1) for b in mine)


def places_of():
    own, x = (lax.axis_index("tp_1"), lax.axis_index("tp_0"))
    return [
        ((x + ahead) % 4) * 2 + core for core in (own, 1 - own) for ahead in (0, 3, 1, 2)
    ]


def first_matmuls(blocks, gate, up, capacity):
    n, tall, _ = blocks[0].shape
    pieces = tall // capacity
    width = pieces * LANES
    depth, cols = gate.shape
    rows = n * capacity
    count = len(blocks)

    def body(*refs):
        ins, (gate_ref, up_ref, out_ref, in_buf, w_buf) = (refs[:count], refs[count:])
        for i, tp in enumerate(places_of()):
            d = pl.ds(pl.multiple_of(tp * width, width), width)
            to = slice(i * width, (i + 1) * width)
            w_buf[to, :cols] = gate_ref[d, :]
            w_buf[to, cols:] = up_ref[d, :]
            for p in range(pieces):
                lanes = slice(i * width + p * LANES, i * width + (p + 1) * LANES)
                in_buf[:, lanes] = ins[i][:, p * capacity : (p + 1) * capacity, :].reshape(rows, LANES)
        both = dot(in_buf[...], w_buf[...])
        g = both[:, :cols]
        out_ref[...] = (g / (1.0 + jnp.exp(-g)) * both[:, cols:]).astype(BF)

    return pl.pallas_call(
        body,
        out_shape=held((rows, cols)),
        in_specs=[VM] * (count + 2),
        out_specs=VM,
        compiler_params=LIMIT,
        scratch_shapes=[pltpu.VMEM((rows, depth), BF), pltpu.VMEM((depth, 2 * cols), BF)],
    )(*near_core([*blocks, gate, up]))


def second_matmul(blocks, down, n, k, per_device, done):
    rows, width = blocks[0].shape
    depth, cols = down.shape
    capacity = rows // n
    count = len(blocks)
    last = k == per_device - 1

    def body(*refs):
        ins, (down_ref, *dones) = (refs[:count], refs[count : count + 1 + len(done)])
        out_ref, in_buf, down_buf = refs[count + 1 + len(done) :]
        for i, tp in enumerate(places_of()):
            to = slice(i * width, (i + 1) * width)
            down_buf[to, :] = down_ref[pl.ds(pl.multiple_of(tp * width, width), width), :]
            in_buf[:, to] = ins[i][...]
        out = dot(in_buf[...], down_buf[...]).reshape(n, capacity, cols).astype(BF)
        if last:
            out_ref[:, expert_at(k, per_device)] = out
            for i, ref in enumerate(dones):
                out_ref[:, expert_at(i, per_device)] = ref[...]
        else:
            out_ref[...] = out

    return pl.pallas_call(
        body,
        out_shape=shape((n, per_device, capacity, cols)) if last else held((n, capacity, cols)),
        in_specs=[VM] * (count + 1 + len(done)),
        out_specs=VM,
        compiler_params=LIMIT,
        scratch_shapes=[pltpu.VMEM((rows, depth), BF), pltpu.VMEM((depth, cols), BF)],
    )(*near_core([*blocks, down, *done]))


def combine(returned, route_ids, route_weights, capacity):
    rows, cols = (route_ids.shape[0], returned.shape[1])
    slots = returned.shape[0]

    def body(ret_ref, ids_ref, w_ref, out_ref):
        total = jnp.zeros((rows, cols), F32)
        for r, slot in enumerate(slot_of(ids_ref, capacity)):
            pick = (iota((rows, slots), 1) == slot).astype(BF)
            total = total + dot(pick, ret_ref[...]) * as_column(w_ref[r : r + 1, :])
        out_ref[...] = total.astype(BF)

    return pl.pallas_call(
        body, out_shape=shape((rows, cols)), in_specs=[VM] * 3, out_specs=VM, compiler_params=LIMIT
    )(*near_core([returned, route_ids.T, route_weights.T]))


def by_target(master, n):
    return master.reshape(n, -1, master.shape[2])


def share(master, index, count, n):
    whole = by_target(master, n)
    size = whole.shape[1] // count
    return lax.dynamic_slice_in_dim(whole, index * size, size, 1)


def ring(x, axis):
    n = lax.axis_size(axis)
    out, ahead, behind = ([(0, x)], x, x)
    for k in range(1, n // 2 + 1):
        ahead = shift(ahead, axis, 1)
        out.append((k, ahead))
        if k <= (n - 1) // 2:
            behind = shift(behind, axis, -1)
            out.append((n - k, behind))
    return out


def assemble(pieces, index, count, per_device):
    n, rows, cols = pieces[0][1].shape
    buffer = jnp.zeros((count, n, rows, cols), BF)
    for back, piece in pieces:
        at = (index - back) % count
        buffer = lax.dynamic_update_slice(buffer, piece[None], (at, 0, 0, 0))
    split = count // per_device
    buffer = buffer.reshape(per_device, split, n, rows, cols).transpose(0, 2, 1, 3, 4)
    return buffer.reshape(per_device, -1, cols)


def one_by_one(pieces, served, index, count, per_device):
    if count == per_device:
        return [p.reshape(-1, p.shape[-1]) for _, p in sorted(pieces, key=lambda q: q[0])]
    return [
        lax.dynamic_index_in_dim(served, (index + per_device - k) % per_device, 0, False)
        for k in range(per_device)
    ]


def on_device(tokens, route_ids, route_weights, ffn_gain, gate_master, up_master, down_master):
    n = lax.axis_size("fs")
    count, index = (lax.axis_size("grp"), lax.axis_index("grp"))
    experts, rows, _ = gate_master.shape
    per_device = experts // n
    groups = experts // GROUP_SIZE
    members = n // groups
    capacity = tokens.shape[0] // (2 * groups)
    size = per_device * rows // count

    def swap(x):
        return lax.all_to_all(x, "fs", split_axis=0, concat_axis=0, tiled=True)

    def neighbour(x, k):
        pairs = [(i, i - i % members + (i + k) % members) for i in range(n)]
        return lax.ppermute(x, "fs", pairs)

    packed = pack_first(
        tokens, route_ids, ffn_gain[None, :], by_target(gate_master, n), n, count, groups
    )
    packed = swap(packed)
    gate, near, named = jnp.split(packed, [size, packed.shape[1] - META], axis=1)
    near = [near] + [neighbour(near, k) for k in range(1, members)]
    if size < rows:
        gain = lax.dynamic_slice_in_dim(ffn_gain, index * size % rows, size)
    else:
        gain = jnp.concatenate([ffn_gain] * (size // rows))
    up = swap((share(up_master, index, count, n) * gain[None, :, None]).astype(BF))
    chosen = select_rows(near, named, per_device, capacity)
    down = swap(share(down_master, index, count, n).astype(BF))
    gate = ring(gate, "grp")
    up = ring(up, "grp")
    down = ring(down, "grp")
    gate_serve = assemble(gate, index, count, per_device)
    up_serve = assemble(up, index, count, per_device)
    down_serve = assemble(down, index, count, per_device)
    gates = one_by_one(gate, gate_serve, index, count, per_device)
    ups = one_by_one(up, up_serve, index, count, per_device)
    downs = one_by_one(down, down_serve, index, count, per_device)
    outs = []
    for k in range(per_device):
        blocks = gather_tp(chosen[k], k % 2)
        hidden = first_matmuls(blocks, gates[k], ups[k], capacity)
        hidden = gather_tp(hidden, k % 2)
        last = k == per_device - 1
        outs.append(second_matmul(hidden, downs[k], n, k, per_device, outs if last else []))
    out = swap(outs[-1])
    mixed = combine(out.reshape(-1, out.shape[-1]), route_ids, route_weights, capacity)
    return (gate_serve, up_serve, down_serve, mixed)


def solution(mesh):
    grp, fs, tp = (mesh.shape["grp"], mesh.shape["fs"], mesh.shape["tp"])
    split = Mesh(mesh.devices.reshape(grp, fs, tp // 2, 2), ("grp", "fs", *TP))
    in_specs = (
        P(("grp", "fs"), None),
        P(("grp", "fs"), None),
        P(("grp", "fs"), None),
        P("fs"),
        P(None, "fs", TP),
        P(None, "fs", TP),
        P(None, "fs", TP),
    )
    out_specs = (
        P(("grp", "fs"), None, TP),
        P(("grp", "fs"), None, TP),
        P(("grp", "fs"), None, TP),
        P(("grp", "fs"), TP),
    )
    return jax.shard_map(on_device, mesh=split, in_specs=in_specs, out_specs=out_specs, check_vma=False)
```

```python
import jax
import jax.numpy as jnp
from jax import lax
from jax.experimental import pallas as pl
from jax.experimental.pallas import tpu as pltpu
from jax.sharding import Mesh
from jax.sharding import PartitionSpec as P


GROUP_SIZE = 8
TP = ("tp_0", "tp_1")
BF = jnp.bfloat16
F32 = jnp.float32
LANES = 128
META = 8
PAIR = 2
LIMIT = pltpu.CompilerParams(vmem_limit_bytes=14 * 2**20)

VM = pl.BlockSpec(memory_space=pltpu.VMEM)
ANY = pl.BlockSpec(memory_space=pl.ANY)


def shift(x, axis, k):
    n = lax.axis_size(axis)
    return lax.ppermute(x, axis, [(i, (i + k) % n) for i in range(n)])


def shape(dims, dtype=BF):
    return jax.ShapeDtypeStruct(dims, dtype)


def held(dims, dtype=BF):
    return pltpu.VMEM(dims, dtype)


def near_core(arrays):
    return [pltpu.with_memory_space_constraint(a, pltpu.VMEM) for a in arrays]


def iota(dims, dim):
    return lax.broadcasted_iota(jnp.int32, dims, dim)


def dot(a, b, dims=((1,), (0,))):
    return lax.dot_general(a, b, (dims, ((), ())), preferred_element_type=F32)


def as_column(row):
    n = row.shape[1]
    same = iota((n, n), 0) == iota((n, n), 1)
    return jnp.sum(jnp.where(same, row, jnp.zeros_like(row)), axis=1, keepdims=True)


def slot_of(ids_ref, capacity):
    rows = ids_ref.shape[1]
    ids = [as_column(ids_ref[r : r + 1, :].astype(F32)) for r in range(2)]
    lane = iota((rows, LANES), 1).astype(F32)
    hits = [lane == i for i in ids]
    before = (iota((rows, rows), 0) > iota((rows, rows), 1)).astype(BF)
    count = dot(before, jnp.where(hits[0] | hits[1], 1.0, 0.0).astype(BF))
    return [
        (i * capacity + jnp.sum(jnp.where(h, count, 0.0), axis=1, keepdims=True)).astype(jnp.int32)
        for i, h in zip(ids, hits)
    ]


def pack_first(tokens, route_ids, gain, gate, up, n, count, groups):
    tokens_n, model = tokens.shape
    _, whole, cols = gate.shape
    size = whole // count
    width = model // lax.axis_size(TP)
    part = tokens_n // groups
    members = n // groups
    each = part // PAIR
    pieces = width // LANES
    gain_rows = gain.shape[1]

    def body(tok_ref, ids_ref, gain_ref, gate_ref, up_ref, out_ref, buf_ref, sems):
        share_of = pl.ds(pl.multiple_of(lax.axis_index("grp") * size, size), size)
        copies = [
            pltpu.make_async_copy(ref.at[:, share_of, :], buf_ref.at[i], sems.at[i])
            for i, ref in enumerate((gate_ref, up_ref))
        ]
        for c in copies:
            c.start()
        tok = tok_ref[...].astype(F32)
        scale = lax.rsqrt(jnp.mean(tok * tok, axis=1, keepdims=True) + 1e-06)
        at = pl.multiple_of(lax.axis_index(TP) * width, width)
        own = (tok_ref[:, pl.ds(at, width)].astype(F32) * scale).astype(BF)
        ids = [as_column(ids_ref[r : r + 1, :].astype(F32)) for r in range(2)]
        group = ids[0].astype(jnp.int32) // GROUP_SIZE
        member = iota((tokens_n, LANES), 1) == group
        before = (iota((tokens_n, tokens_n), 0) > iota((tokens_n, tokens_n), 1)).astype(BF)
        count_before = dot(before, jnp.where(member, 1.0, 0.0).astype(BF))
        rank = jnp.sum(jnp.where(member, count_before, 0.0), axis=1, keepdims=True)
        place = iota((tokens_n, tokens_n), 1) == group * part + rank.astype(jnp.int32)
        ordered = dot(jnp.where(place, 1.0, 0.0).astype(BF), own, ((0,), (0,))).astype(BF)
        local = [i - (group * GROUP_SIZE).astype(F32) for i in ids]
        named = [jnp.sum(jnp.where(place, i, 0.0), axis=0, keepdims=True) for i in local]
        named = jnp.concatenate(named + [jnp.zeros((META - 2, tokens_n), F32)], axis=0)
        for j in range(n):
            a = j // members
            first = a * part + j % PAIR * each
            for p in range(pieces):
                to = 2 * size + p * each
                out_ref[j, to : to + each, :] = ordered[first : first + each, p * LANES : (p + 1) * LANES]
            piece = named[:, a * part : (a + 1) * part]
            piece = jnp.concatenate([piece, jnp.zeros((META, LANES - part), F32)], axis=1)
            out_ref[j, 2 * size + pieces * each :, :] = piece.astype(BF)
        column = as_column(gain_ref[...])
        if size >= gain_rows:
            column = jnp.concatenate([column] * (size // gain_rows), axis=0)
        else:
            skip = lax.axis_index("grp") * size % gain_rows
            row = iota((size, gain_rows), 1) == iota((size, gain_rows), 0) + skip
            column = jnp.sum(jnp.where(row, gain_ref[...], 0.0), axis=1, keepdims=True)
        for i, c in enumerate(copies):
            c.wait()
            for j in range(n):
                out_ref[j, i * size : (i + 1) * size, :] = (buf_ref[i, j] * column).astype(BF)

    return pl.pallas_call(
        body,
        out_shape=shape((n, 2 * size + pieces * each + META, cols)),
        in_specs=[VM, VM, VM, ANY, ANY],
        out_specs=VM,
        scratch_shapes=[pltpu.VMEM((2, n, size, cols), F32), pltpu.SemaphoreType.DMA((2,))],
    )(tokens, route_ids.T, gain, gate, up)


def select_rows(blocks, named, members, pieces, per_device, capacity):
    n, tall, _ = blocks[0].shape
    each = tall // pieces
    part = PAIR * each

    def body(*refs):
        ins, (named_ref, *outs) = (refs[:PAIR], refs[PAIR : PAIR + 1 + per_device])
        row_ref = refs[-1]
        here = lax.axis_index("fs") % members
        for k in range(PAIR):
            to = pl.ds(pl.multiple_of((here + k) % PAIR * each, each), each)
            for p in range(pieces):
                row_ref[:, to, p * LANES : (p + 1) * LANES] = ins[k][:, p * each : (p + 1) * each, :]
        named_rows = named_ref[...].astype(F32)
        one, two = [
            jnp.concatenate([named_rows[j, r : r + 1, :part] for j in range(n)], axis=0) for r in range(2)
        ]
        earlier = (iota((part, part), 0) < iota((part, part), 1)).astype(BF)
        slot = iota((capacity, part), 0).astype(F32)
        ranks = []
        for k in range(per_device):
            e = here * per_device + expert_at(k, per_device)
            hit = (one == e.astype(F32)) | (two == e.astype(F32))
            rank = dot(jnp.where(hit, 1.0, 0.0).astype(BF), earlier)
            ranks.append(jnp.where(hit, rank, -1.0))
        for j in range(n):
            pick = [jnp.where(slot == ranks[k][j : j + 1], 1.0, 0.0) for k in range(per_device)]
            got = dot(jnp.concatenate(pick, axis=0).astype(BF), row_ref[j]).astype(BF)
            for k in range(per_device):
                for p in range(pieces):
                    outs[k][j, p * capacity : (p + 1) * capacity, :] = got[
                        k * capacity : (k + 1) * capacity, p * LANES : (p + 1) * LANES
                    ]

    return pl.pallas_call(
        body,
        out_shape=tuple(held((n, pieces * capacity, LANES)) for _ in range(per_device)),
        in_specs=[VM] * (PAIR + 1),
        out_specs=tuple(VM for _ in range(per_device)),
        compiler_params=LIMIT,
        scratch_shapes=[pltpu.VMEM((n, part, pieces * LANES), BF)],
    )(*near_core([*blocks, named]))


def expert_at(k, per_device):
    return (lax.axis_index("grp") + per_device - k) % per_device


def gather_tp(x, back):
    left, right = (shift(x, "tp_0", 1), shift(x, "tp_0", -1))
    across = shift(right, "tp_0", -1) if back else shift(left, "tp_0", 1)
    mine = (x, left, right, across)
    return mine + tuple(shift(b, "tp_1", 1) for b in mine)


def places_of():
    own, x = (lax.axis_index("tp_1"), lax.axis_index("tp_0"))
    return [
        ((x + ahead) % 4) * 2 + core for core in (own, 1 - own) for ahead in (0, 3, 1, 2)
    ]


def first_matmuls(blocks, weights, capacity):
    n, tall, _ = blocks[0].shape
    pieces = tall // capacity
    width = pieces * LANES
    _, both_rows, cols = weights.shape
    each = both_rows // 2
    depth = n * each
    rows = n * capacity
    count = len(blocks)

    def body(*refs):
        ins, (weight_ref, out_ref, in_buf, w_buf) = (refs[:count], refs[count:])
        for i, tp in enumerate(places_of()):
            for q in range(width // each):
                to = slice(i * width + q * each, i * width + (q + 1) * each)
                from_fs = tp * (width // each) + q
                w_buf[to, :cols] = weight_ref[from_fs, :each, :]
                w_buf[to, cols:] = weight_ref[from_fs, each:, :]
            for p in range(pieces):
                lanes = slice(i * width + p * LANES, i * width + (p + 1) * LANES)
                in_buf[:, lanes] = ins[i][:, p * capacity : (p + 1) * capacity, :].reshape(rows, LANES)
        both = dot(in_buf[...], w_buf[...])
        g = both[:, :cols]
        out_ref[...] = (g / (1.0 + jnp.exp(-g)) * both[:, cols:]).astype(BF)

    return pl.pallas_call(
        body,
        out_shape=held((rows, cols)),
        in_specs=[VM] * (count + 1),
        out_specs=VM,
        compiler_params=LIMIT,
        scratch_shapes=[pltpu.VMEM((rows, depth), BF), pltpu.VMEM((depth, 2 * cols), BF)],
    )(*near_core([*blocks, weights]))


def second_matmul(blocks, down, n, k, per_device, done):
    rows, width = blocks[0].shape
    depth, cols = down.shape
    capacity = rows // n
    count = len(blocks)
    last = k == per_device - 1

    def body(*refs):
        ins, (down_ref, *dones) = (refs[:count], refs[count : count + 1 + len(done)])
        out_ref, in_buf, down_buf = refs[count + 1 + len(done) :]
        for i, tp in enumerate(places_of()):
            to = slice(i * width, (i + 1) * width)
            down_buf[to, :] = down_ref[pl.ds(pl.multiple_of(tp * width, width), width), :]
            in_buf[:, to] = ins[i][...]
        out = dot(in_buf[...], down_buf[...]).reshape(n, capacity, cols).astype(BF)
        if last:
            out_ref[:, expert_at(k, per_device)] = out
            for i, ref in enumerate(dones):
                out_ref[:, expert_at(i, per_device)] = ref[...]
        else:
            out_ref[...] = out

    return pl.pallas_call(
        body,
        out_shape=shape((n, per_device, capacity, cols)) if last else held((n, capacity, cols)),
        in_specs=[VM] * (count + 1 + len(done)),
        out_specs=VM,
        compiler_params=LIMIT,
        scratch_shapes=[pltpu.VMEM((rows, depth), BF), pltpu.VMEM((depth, cols), BF)],
    )(*near_core([*blocks, down, *done]))


def weigh(route_ids, route_weights, slots, capacity):
    rows = route_ids.shape[0]

    def body(ids_ref, w_ref, out_ref):
        lane = iota((rows, slots), 1)
        total = jnp.zeros((rows, slots), F32)
        for r, slot in enumerate(slot_of(ids_ref, capacity)):
            total = jnp.where(lane == slot, as_column(w_ref[r : r + 1, :]), total)
        high = total.astype(BF)
        out_ref[0] = high
        out_ref[1] = (total - high.astype(F32)).astype(BF)

    return pl.pallas_call(
        body,
        out_shape=held((2, rows, slots)),
        in_specs=[VM] * 2,
        out_specs=VM,
        compiler_params=LIMIT,
    )(route_ids.T, route_weights.T)


def combine(returned, picks):
    def body(ret_ref, pick_ref, out_ref):
        out_ref[...] = (dot(pick_ref[0], ret_ref[...]) + dot(pick_ref[1], ret_ref[...])).astype(BF)

    return pl.pallas_call(
        body,
        out_shape=shape((picks.shape[1], returned.shape[1])),
        in_specs=[VM] * 2,
        out_specs=VM,
        compiler_params=LIMIT,
    )(*near_core([returned, picks]))


def by_target(master, n):
    return master.reshape(n, -1, master.shape[2])


def share(master, index, count, n):
    whole = by_target(master, n)
    size = whole.shape[1] // count
    return lax.dynamic_slice_in_dim(whole, index * size, size, 1)


def ring(x, axis):
    n = lax.axis_size(axis)
    out, ahead, behind = ([(0, x)], x, x)
    for k in range(1, n // 2 + 1):
        ahead = shift(ahead, axis, 1)
        out.append((k, ahead))
        if k <= (n - 1) // 2:
            behind = shift(behind, axis, -1)
            out.append((n - k, behind))
    return out


def assemble(pieces, index, count, per_device):
    n, rows, cols = pieces[0][1].shape
    buffer = jnp.zeros((count, n, rows, cols), BF)
    for back, piece in pieces:
        at = (index - back) % count
        buffer = lax.dynamic_update_slice(buffer, piece[None], (at, 0, 0, 0))
    split = count // per_device
    buffer = buffer.reshape(per_device, split, n, rows, cols).transpose(0, 2, 1, 3, 4)
    return buffer.reshape(per_device, -1, cols)


def one_by_one(pieces, served, index, count, n, per_device):
    if count == per_device:
        return [p for _, p in sorted(pieces, key=lambda q: q[0])]
    out = []
    for k in range(per_device):
        e = (index + per_device - k) % per_device
        own = [lax.dynamic_index_in_dim(m, e, 0, False) for m in served]
        out.append(jnp.concatenate([m.reshape(n, -1, m.shape[-1]) for m in own], axis=1))
    return out


def on_device(tokens, route_ids, route_weights, ffn_gain, gate_master, up_master, down_master):
    n = lax.axis_size("fs")
    count, index = (lax.axis_size("grp"), lax.axis_index("grp"))
    experts, rows, _ = gate_master.shape
    per_device = experts // n
    groups = experts // GROUP_SIZE
    members = n // groups
    capacity = tokens.shape[0] // (2 * groups)
    pieces = tokens.shape[1] // lax.axis_size(TP) // LANES
    size = per_device * rows // count

    def swap(x):
        return lax.all_to_all(x, "fs", split_axis=0, concat_axis=0, tiled=True)

    packed = pack_first(
        tokens,
        route_ids,
        ffn_gain[None, :],
        by_target(gate_master, n),
        by_target(up_master, n),
        n,
        count,
        groups,
    )
    packed = swap(packed)
    both, own, named = jnp.split(packed, [2 * size, packed.shape[1] - META], axis=1)
    other = lax.ppermute(own, "fs", [(i, i - i % PAIR + (i + 1) % PAIR) for i in range(n)])
    chosen = select_rows([own, other], named, members, pieces, per_device, capacity)
    down = swap(share(down_master, index, count, n).astype(BF))
    both = ring(both, "grp")
    down = ring(down, "grp")
    gate_serve = assemble([(k, p[:, :size]) for k, p in both], index, count, per_device)
    up_serve = assemble([(k, p[:, size:]) for k, p in both], index, count, per_device)
    down_serve = assemble(down, index, count, per_device)
    firsts = one_by_one(both, [gate_serve, up_serve], index, count, n, per_device)
    seconds = one_by_one(down, [down_serve], index, count, n, per_device)
    outs = []
    for k in range(per_device):
        blocks = gather_tp(chosen[k], k % 2)
        hidden = first_matmuls(blocks, firsts[k], capacity)
        hidden = gather_tp(hidden, k % 2)
        last = k == per_device - 1
        weights = seconds[k].reshape(-1, seconds[k].shape[-1])
        outs.append(second_matmul(hidden, weights, n, k, per_device, outs if last else []))
    picks = weigh(route_ids, route_weights, experts * capacity, capacity)
    out = swap(outs[-1])
    mixed = combine(out.reshape(-1, out.shape[-1]), picks)
    return (gate_serve, up_serve, down_serve, mixed)


def solution(mesh):
    grp, fs, tp = (mesh.shape["grp"], mesh.shape["fs"], mesh.shape["tp"])
    split = Mesh(mesh.devices.reshape(grp, fs, tp // 2, 2), ("grp", "fs", *TP))
    in_specs = (
        P(("grp", "fs"), None),
        P(("grp", "fs"), None),
        P(("grp", "fs"), None),
        P("fs"),
        P(None, "fs", TP),
        P(None, "fs", TP),
        P(None, "fs", TP),
    )
    out_specs = (
        P(("grp", "fs"), None, TP),
        P(("grp", "fs"), None, TP),
        P(("grp", "fs"), None, TP),
        P(("grp", "fs"), TP),
    )
    return jax.shard_map(on_device, mesh=split, in_specs=in_specs, out_specs=out_specs, check_vma=False)
```

```python
import jax
import jax.numpy as jnp
from jax import lax
from jax.experimental import pallas as pl
from jax.experimental.pallas import tpu as pltpu
from jax.sharding import Mesh
from jax.sharding import PartitionSpec as P


GROUP_SIZE = 8
TP = ("tp_0", "tp_1")
BF = jnp.bfloat16
F32 = jnp.float32
LANES = 128
META = 8
PAIR = 2
LIMIT = pltpu.CompilerParams(vmem_limit_bytes=14 * 2**20)

VM = pl.BlockSpec(memory_space=pltpu.VMEM)
ANY = pl.BlockSpec(memory_space=pl.ANY)


def shift(x, axis, k):
    n = lax.axis_size(axis)
    return lax.ppermute(x, axis, [(i, (i + k) % n) for i in range(n)])


def shape(dims, dtype=BF):
    return jax.ShapeDtypeStruct(dims, dtype)


def held(dims, dtype=BF):
    return pltpu.VMEM(dims, dtype)


def near_core(arrays):
    return [pltpu.with_memory_space_constraint(a, pltpu.VMEM) for a in arrays]


def iota(dims, dim):
    return lax.broadcasted_iota(jnp.int32, dims, dim)


def dot(a, b, dims=((1,), (0,))):
    return lax.dot_general(a, b, (dims, ((), ())), preferred_element_type=F32)


def as_column(row):
    n = row.shape[1]
    same = iota((n, n), 0) == iota((n, n), 1)
    return jnp.sum(jnp.where(same, row, jnp.zeros_like(row)), axis=1, keepdims=True)


def slot_of(ids_ref, capacity):
    rows = ids_ref.shape[1]
    ids = [as_column(ids_ref[r : r + 1, :].astype(F32)) for r in range(2)]
    lane = iota((rows, LANES), 1).astype(F32)
    hits = [lane == i for i in ids]
    before = (iota((rows, rows), 0) > iota((rows, rows), 1)).astype(BF)
    count = dot(before, jnp.where(hits[0] | hits[1], 1.0, 0.0).astype(BF))
    return [
        (i * capacity + jnp.sum(jnp.where(h, count, 0.0), axis=1, keepdims=True)).astype(jnp.int32)
        for i, h in zip(ids, hits)
    ]


def pack_first(tokens, route_ids, gain, gate, up, n, count, groups):
    tokens_n, model = tokens.shape
    _, whole, cols = gate.shape
    size = whole // count
    width = model // lax.axis_size(TP)
    part = tokens_n // groups
    members = n // groups
    each = part // PAIR
    pieces = width // LANES
    gain_rows = gain.shape[1]

    def body(tok_ref, ids_ref, gain_ref, gate_ref, up_ref, out_ref, buf_ref, sems):
        share_of = pl.ds(pl.multiple_of(lax.axis_index("grp") * size, size), size)
        copies = [
            pltpu.make_async_copy(ref.at[:, share_of, :], buf_ref.at[i], sems.at[i])
            for i, ref in enumerate((gate_ref, up_ref))
        ]
        for c in copies:
            c.start()
        tok = tok_ref[...].astype(F32)
        scale = lax.rsqrt(jnp.mean(tok * tok, axis=1, keepdims=True) + 1e-06)
        at = pl.multiple_of(lax.axis_index(TP) * width, width)
        own = (tok_ref[:, pl.ds(at, width)].astype(F32) * scale).astype(BF)
        ids = [as_column(ids_ref[r : r + 1, :].astype(F32)) for r in range(2)]
        group = ids[0].astype(jnp.int32) // GROUP_SIZE
        member = iota((tokens_n, LANES), 1) == group
        before = (iota((tokens_n, tokens_n), 0) > iota((tokens_n, tokens_n), 1)).astype(BF)
        count_before = dot(before, jnp.where(member, 1.0, 0.0).astype(BF))
        rank = jnp.sum(jnp.where(member, count_before, 0.0), axis=1, keepdims=True)
        place = iota((tokens_n, tokens_n), 1) == group * part + rank.astype(jnp.int32)
        ordered = dot(jnp.where(place, 1.0, 0.0).astype(BF), own, ((0,), (0,))).astype(BF)
        local = [i - (group * GROUP_SIZE).astype(F32) for i in ids]
        named = [jnp.sum(jnp.where(place, i, 0.0), axis=0, keepdims=True) for i in local]
        named = jnp.concatenate(named + [jnp.zeros((META - 2, tokens_n), F32)], axis=0)
        for j in range(n):
            a = j // members
            first = a * part + j % PAIR * each
            for p in range(pieces):
                to = 2 * size + p * each
                out_ref[j, to : to + each, :] = ordered[first : first + each, p * LANES : (p + 1) * LANES]
            piece = named[:, a * part : (a + 1) * part]
            piece = jnp.concatenate([piece, jnp.zeros((META, LANES - part), F32)], axis=1)
            out_ref[j, 2 * size + pieces * each :, :] = piece.astype(BF)
        column = as_column(gain_ref[...])
        if size >= gain_rows:
            column = jnp.concatenate([column] * (size // gain_rows), axis=0)
        else:
            skip = lax.axis_index("grp") * size % gain_rows
            row = iota((size, gain_rows), 1) == iota((size, gain_rows), 0) + skip
            column = jnp.sum(jnp.where(row, gain_ref[...], 0.0), axis=1, keepdims=True)
        for i, c in enumerate(copies):
            c.wait()
            for j in range(n):
                out_ref[j, i * size : (i + 1) * size, :] = (buf_ref[i, j] * column).astype(BF)

    return pl.pallas_call(
        body,
        out_shape=shape((n, 2 * size + pieces * each + META, cols)),
        in_specs=[VM, VM, VM, ANY, ANY],
        out_specs=VM,
        scratch_shapes=[pltpu.VMEM((2, n, size, cols), F32), pltpu.SemaphoreType.DMA((2,))],
    )(tokens, route_ids.T, gain, gate, up)


def unpack(packed, cuts):
    n, tall, cols = packed.shape
    ends = [0, *cuts, tall]
    parts = list(zip(ends[:-1], ends[1:]))

    def body(packed_ref, *refs):
        sems = refs[-1]
        copies = [
            pltpu.make_async_copy(packed_ref.at[:, a:b, :], refs[i], sems.at[i])
            for i, (a, b) in enumerate(parts)
        ]
        for c in copies:
            c.start()
        for c in copies:
            c.wait()

    return pl.pallas_call(
        body,
        out_shape=tuple(shape((n, b - a, cols)) for a, b in parts),
        in_specs=[ANY],
        out_specs=tuple(VM for _ in parts),
        compiler_params=LIMIT,
        scratch_shapes=[pltpu.SemaphoreType.DMA((len(parts),))],
    )(packed)


def select_rows(blocks, named, members, pieces, per_device, capacity):
    n, tall, _ = blocks[0].shape
    each = tall // pieces
    part = PAIR * each

    def body(*refs):
        ins, (named_ref, *outs) = (refs[:PAIR], refs[PAIR : PAIR + 1 + per_device])
        row_ref = refs[-1]
        here = lax.axis_index("fs") % members
        for k in range(PAIR):
            to = pl.ds(pl.multiple_of((here + k) % PAIR * each, each), each)
            for p in range(pieces):
                row_ref[:, to, p * LANES : (p + 1) * LANES] = ins[k][:, p * each : (p + 1) * each, :]
        named_rows = named_ref[...].astype(F32)
        one, two = [
            jnp.concatenate([named_rows[j, r : r + 1, :part] for j in range(n)], axis=0) for r in range(2)
        ]
        earlier = (iota((part, part), 0) < iota((part, part), 1)).astype(BF)
        slot = iota((capacity, part), 0).astype(F32)
        ranks = []
        for k in range(per_device):
            e = here * per_device + expert_at(k, per_device)
            hit = (one == e.astype(F32)) | (two == e.astype(F32))
            rank = dot(jnp.where(hit, 1.0, 0.0).astype(BF), earlier)
            ranks.append(jnp.where(hit, rank, -1.0))
        for j in range(n):
            pick = [jnp.where(slot == ranks[k][j : j + 1], 1.0, 0.0) for k in range(per_device)]
            got = dot(jnp.concatenate(pick, axis=0).astype(BF), row_ref[j]).astype(BF)
            for k in range(per_device):
                for p in range(pieces):
                    outs[k][j, p * capacity : (p + 1) * capacity, :] = got[
                        k * capacity : (k + 1) * capacity, p * LANES : (p + 1) * LANES
                    ]

    return pl.pallas_call(
        body,
        out_shape=tuple(held((n, pieces * capacity, LANES)) for _ in range(per_device)),
        in_specs=[VM] * (PAIR + 1),
        out_specs=tuple(VM for _ in range(per_device)),
        compiler_params=LIMIT,
        scratch_shapes=[pltpu.VMEM((n, part, pieces * LANES), BF)],
    )(*near_core([*blocks, named]))


def expert_at(k, per_device):
    return (lax.axis_index("grp") + per_device - k) % per_device


def gather_tp(x, back):
    left, right = (shift(x, "tp_0", 1), shift(x, "tp_0", -1))
    across = shift(right, "tp_0", -1) if back else shift(left, "tp_0", 1)
    mine = (x, left, right)
    theirs = tuple(shift(b, "tp_1", 1) for b in mine)
    return mine + (across,) + theirs + (shift(across, "tp_1", 1),)


def places_of():
    own, x = (lax.axis_index("tp_1"), lax.axis_index("tp_0"))
    return [
        ((x + ahead) % 4) * 2 + core for core in (own, 1 - own) for ahead in (0, 3, 1, 2)
    ]


def first_matmuls(blocks, weights, capacity):
    n, tall, _ = blocks[0].shape
    pieces = tall // capacity
    width = pieces * LANES
    _, both_rows, cols = weights.shape
    each = both_rows // 2
    depth = n * each
    rows = n * capacity
    count = len(blocks)

    def body(*refs):
        ins, (weight_ref, out_ref, in_buf, w_buf) = (refs[:count], refs[count:])
        for i, tp in enumerate(places_of()):
            for q in range(width // each):
                to = slice(i * width + q * each, i * width + (q + 1) * each)
                from_fs = tp * (width // each) + q
                w_buf[to, :cols] = weight_ref[from_fs, :each, :]
                w_buf[to, cols:] = weight_ref[from_fs, each:, :]
            for p in range(pieces):
                lanes = slice(i * width + p * LANES, i * width + (p + 1) * LANES)
                in_buf[:, lanes] = ins[i][:, p * capacity : (p + 1) * capacity, :].reshape(rows, LANES)
        both = dot(in_buf[...], w_buf[...])
        g = both[:, :cols]
        out_ref[...] = (g / (1.0 + jnp.exp(-g)) * both[:, cols:]).astype(BF)

    return pl.pallas_call(
        body,
        out_shape=held((rows, cols)),
        in_specs=[VM] * (count + 1),
        out_specs=VM,
        compiler_params=LIMIT,
        scratch_shapes=[pltpu.VMEM((rows, depth), BF), pltpu.VMEM((depth, 2 * cols), BF)],
    )(*near_core([*blocks, weights]))


def second_matmul(blocks, down, n, k, per_device, done):
    rows, width = blocks[0].shape
    depth, cols = down.shape
    capacity = rows // n
    count = len(blocks)
    last = k == per_device - 1

    def body(*refs):
        ins, (down_ref, *dones) = (refs[:count], refs[count : count + 1 + len(done)])
        out_ref, in_buf, down_buf = refs[count + 1 + len(done) :]
        for i, tp in enumerate(places_of()):
            to = slice(i * width, (i + 1) * width)
            down_buf[to, :] = down_ref[pl.ds(pl.multiple_of(tp * width, width), width), :]
            in_buf[:, to] = ins[i][...]
        out = dot(in_buf[...], down_buf[...]).reshape(n, capacity, cols).astype(BF)
        if last:
            out_ref[:, expert_at(k, per_device)] = out
            for i, ref in enumerate(dones):
                out_ref[:, expert_at(i, per_device)] = ref[...]
        else:
            out_ref[...] = out

    return pl.pallas_call(
        body,
        out_shape=shape((n, per_device, capacity, cols)) if last else held((n, capacity, cols)),
        in_specs=[VM] * (count + 1 + len(done)),
        out_specs=VM,
        compiler_params=LIMIT,
        scratch_shapes=[pltpu.VMEM((rows, depth), BF), pltpu.VMEM((depth, cols), BF)],
    )(*near_core([*blocks, down, *done]))


def weigh(route_ids, route_weights, slots, capacity):
    rows = route_ids.shape[0]

    def body(ids_ref, w_ref, out_ref):
        lane = iota((rows, slots), 1)
        total = jnp.zeros((rows, slots), F32)
        for r, slot in enumerate(slot_of(ids_ref, capacity)):
            total = jnp.where(lane == slot, as_column(w_ref[r : r + 1, :]), total)
        high = total.astype(BF)
        out_ref[0] = high
        out_ref[1] = (total - high.astype(F32)).astype(BF)

    return pl.pallas_call(
        body,
        out_shape=held((2, rows, slots)),
        in_specs=[VM] * 2,
        out_specs=VM,
        compiler_params=LIMIT,
    )(route_ids.T, route_weights.T)


def combine(returned, picks):
    def body(ret_ref, pick_ref, out_ref):
        out_ref[...] = (dot(pick_ref[0], ret_ref[...]) + dot(pick_ref[1], ret_ref[...])).astype(BF)

    return pl.pallas_call(
        body,
        out_shape=shape((picks.shape[1], returned.shape[1])),
        in_specs=[VM] * 2,
        out_specs=VM,
        compiler_params=LIMIT,
    )(*near_core([returned, picks]))


def by_target(master, n):
    return master.reshape(n, -1, master.shape[2])


def share(master, index, count, n):
    whole = by_target(master, n)
    size = whole.shape[1] // count
    return lax.dynamic_slice_in_dim(whole, index * size, size, 1)


def ring(x, axis):
    n = lax.axis_size(axis)
    out, ahead, behind = ([(0, x)], x, x)
    for k in range(1, n // 2 + 1):
        ahead = shift(ahead, axis, 1)
        out.append((k, ahead))
        if k <= (n - 1) // 2:
            behind = shift(behind, axis, -1)
            out.append((n - k, behind))
    return out


def assemble(pieces, index, count, per_device):
    n, rows, cols = pieces[0][1].shape
    buffer = jnp.zeros((count, n, rows, cols), BF)
    for back, piece in pieces:
        at = (index - back) % count
        buffer = lax.dynamic_update_slice(buffer, piece[None], (at, 0, 0, 0))
    split = count // per_device
    buffer = buffer.reshape(per_device, split, n, rows, cols).transpose(0, 2, 1, 3, 4)
    return buffer.reshape(per_device, -1, cols)


def one_by_one(pieces, served, index, count, n, per_device):
    if count == per_device:
        return [p for _, p in sorted(pieces, key=lambda q: q[0])]
    out = []
    for k in range(per_device):
        e = (index + per_device - k) % per_device
        own = [lax.dynamic_index_in_dim(m, e, 0, False) for m in served]
        out.append(jnp.concatenate([m.reshape(n, -1, m.shape[-1]) for m in own], axis=1))
    return out


def on_device(tokens, route_ids, route_weights, ffn_gain, gate_master, up_master, down_master):
    n = lax.axis_size("fs")
    count, index = (lax.axis_size("grp"), lax.axis_index("grp"))
    experts, rows, _ = gate_master.shape
    per_device = experts // n
    groups = experts // GROUP_SIZE
    members = n // groups
    capacity = tokens.shape[0] // (2 * groups)
    pieces = tokens.shape[1] // lax.axis_size(TP) // LANES
    size = per_device * rows // count

    def swap(x):
        return lax.all_to_all(x, "fs", split_axis=0, concat_axis=0, tiled=True)

    packed = pack_first(
        tokens,
        route_ids,
        ffn_gain[None, :],
        by_target(gate_master, n),
        by_target(up_master, n),
        n,
        count,
        groups,
    )
    packed = swap(packed)
    both, own, named = unpack(packed, [2 * size, packed.shape[1] - META])
    other = lax.ppermute(own, "fs", [(i, i - i % PAIR + (i + 1) % PAIR) for i in range(n)])
    chosen = select_rows([own, other], named, members, pieces, per_device, capacity)
    down = swap(share(down_master, index, count, n).astype(BF))
    both = ring(both, "grp")
    down = ring(down, "grp")
    gate_serve = assemble([(k, p[:, :size]) for k, p in both], index, count, per_device)
    up_serve = assemble([(k, p[:, size:]) for k, p in both], index, count, per_device)
    down_serve = assemble(down, index, count, per_device)
    firsts = one_by_one(both, [gate_serve, up_serve], index, count, n, per_device)
    seconds = one_by_one(down, [down_serve], index, count, n, per_device)
    outs = []
    for k in range(per_device):
        blocks = gather_tp(chosen[k], k % 2)
        hidden = first_matmuls(blocks, firsts[k], capacity)
        hidden = gather_tp(hidden, k % 2)
        last = k == per_device - 1
        weights = seconds[k].reshape(-1, seconds[k].shape[-1])
        outs.append(second_matmul(hidden, weights, n, k, per_device, outs if last else []))
    picks = weigh(route_ids, route_weights, experts * capacity, capacity)
    out = swap(outs[-1])
    mixed = combine(out.reshape(-1, out.shape[-1]), picks)
    return (gate_serve, up_serve, down_serve, mixed)


def solution(mesh):
    grp, fs, tp = (mesh.shape["grp"], mesh.shape["fs"], mesh.shape["tp"])
    split = Mesh(mesh.devices.reshape(grp, fs, tp // 2, 2), ("grp", "fs", *TP))
    in_specs = (
        P(("grp", "fs"), None),
        P(("grp", "fs"), None),
        P(("grp", "fs"), None),
        P("fs"),
        P(None, "fs", TP),
        P(None, "fs", TP),
        P(None, "fs", TP),
    )
    out_specs = (
        P(("grp", "fs"), None, TP),
        P(("grp", "fs"), None, TP),
        P(("grp", "fs"), None, TP),
        P(("grp", "fs"), TP),
    )
    return jax.shard_map(on_device, mesh=split, in_specs=in_specs, out_specs=out_specs, check_vma=False)
```

```python
import jax
import jax.numpy as jnp
from jax import lax
from jax.experimental import pallas as pl
from jax.experimental.pallas import tpu as pltpu
from jax.sharding import Mesh
from jax.sharding import PartitionSpec as P


GROUP_SIZE = 8
TP = ("tp_0", "tp_1")
BF = jnp.bfloat16
F32 = jnp.float32
LANES = 128
META = 8
LIMIT = pltpu.CompilerParams(vmem_limit_bytes=14 * 2**20)

VM = pl.BlockSpec(memory_space=pltpu.VMEM)
ANY = pl.BlockSpec(memory_space=pl.ANY)


def shift(x, axis, k):
    n = lax.axis_size(axis)
    return lax.ppermute(x, axis, [(i, (i + k) % n) for i in range(n)])


def shape(dims, dtype=BF):
    return jax.ShapeDtypeStruct(dims, dtype)


def held(dims, dtype=BF):
    return pltpu.VMEM(dims, dtype)


def near_core(arrays):
    return [pltpu.with_memory_space_constraint(a, pltpu.VMEM) for a in arrays]


def iota(dims, dim):
    return lax.broadcasted_iota(jnp.int32, dims, dim)


def dot(a, b, dims=((1,), (0,))):
    return lax.dot_general(a, b, (dims, ((), ())), preferred_element_type=F32)


def as_column(row):
    n = row.shape[1]
    same = iota((n, n), 0) == iota((n, n), 1)
    return jnp.sum(jnp.where(same, row, jnp.zeros_like(row)), axis=1, keepdims=True)


def slot_of(ids_ref, capacity):
    rows = ids_ref.shape[1]
    ids = [as_column(ids_ref[r : r + 1, :].astype(F32)) for r in range(2)]
    lane = iota((rows, LANES), 1).astype(F32)
    hits = [lane == i for i in ids]
    before = (iota((rows, rows), 0) > iota((rows, rows), 1)).astype(BF)
    count = dot(before, jnp.where(hits[0] | hits[1], 1.0, 0.0).astype(BF))
    return [
        (i * capacity + jnp.sum(jnp.where(h, count, 0.0), axis=1, keepdims=True)).astype(jnp.int32)
        for i, h in zip(ids, hits)
    ]


def pack_first(tokens, route_ids, gain, gate, n, count, groups):
    tokens_n, model = tokens.shape
    _, whole, cols = gate.shape
    size = whole // count
    width = model // lax.axis_size(TP)
    part = tokens_n // groups
    members = n // groups
    each = part // members
    pieces = width // LANES
    gain_rows = gain.shape[1]

    def body(tok_ref, ids_ref, gain_ref, gate_ref, out_ref, buf_ref, sem):
        start = pl.multiple_of(lax.axis_index("grp") * size, size)
        copy = pltpu.make_async_copy(gate_ref.at[:, pl.ds(start, size), :], buf_ref, sem)
        copy.start()
        tok = tok_ref[...].astype(F32)
        scale = lax.rsqrt(jnp.mean(tok * tok, axis=1, keepdims=True) + 1e-06)
        at = pl.multiple_of(lax.axis_index(TP) * width, width)
        own = (tok_ref[:, pl.ds(at, width)].astype(F32) * scale).astype(BF)
        ids = [as_column(ids_ref[r : r + 1, :].astype(F32)) for r in range(2)]
        group = ids[0].astype(jnp.int32) // GROUP_SIZE
        member = iota((tokens_n, LANES), 1) == group
        before = (iota((tokens_n, tokens_n), 0) > iota((tokens_n, tokens_n), 1)).astype(BF)
        count_before = dot(before, jnp.where(member, 1.0, 0.0).astype(BF))
        rank = jnp.sum(jnp.where(member, count_before, 0.0), axis=1, keepdims=True)
        place = iota((tokens_n, tokens_n), 1) == group * part + rank.astype(jnp.int32)
        ordered = dot(jnp.where(place, 1.0, 0.0).astype(BF), own, ((0,), (0,))).astype(BF)
        local = [i - (group * GROUP_SIZE).astype(F32) for i in ids]
        named = [jnp.sum(jnp.where(place, i, 0.0), axis=0, keepdims=True) for i in local]
        named = jnp.concatenate(named + [jnp.zeros((META - 2, tokens_n), F32)], axis=0)
        for j in range(n):
            first = j * each
            for p in range(pieces):
                to = size + p * each
                out_ref[j, to : to + each, :] = ordered[first : first + each, p * LANES : (p + 1) * LANES]
            a = j // members
            piece = named[:, a * part : (a + 1) * part]
            piece = jnp.concatenate([piece, jnp.zeros((META, LANES - part), F32)], axis=1)
            out_ref[j, size + pieces * each :, :] = piece.astype(BF)
        column = as_column(gain_ref[...])
        if size >= gain_rows:
            column = jnp.concatenate([column] * (size // gain_rows), axis=0)
        else:
            skip = lax.axis_index("grp") * size % gain_rows
            row = iota((size, gain_rows), 1) == iota((size, gain_rows), 0) + skip
            column = jnp.sum(jnp.where(row, gain_ref[...], 0.0), axis=1, keepdims=True)
        copy.wait()
        for j in range(n):
            out_ref[j, :size, :] = (buf_ref[j] * column).astype(BF)

    return pl.pallas_call(
        body,
        out_shape=shape((n, size + pieces * each + META, cols)),
        in_specs=[VM, VM, VM, ANY],
        out_specs=VM,
        scratch_shapes=[pltpu.VMEM((n, size, cols), F32), pltpu.SemaphoreType.DMA],
    )(tokens, route_ids.T, gain, gate)


def select_rows(blocks, named, per_device, capacity):
    members = len(blocks)
    n, tall, _ = blocks[0].shape
    pieces = 2 * LANES // LANES
    each = tall // pieces
    part = members * each

    def body(*refs):
        ins, (named_ref, *outs) = (refs[:members], refs[members : members + 1 + per_device])
        row_ref = refs[-1]
        here = lax.axis_index("fs") % members
        for k in range(members):
            back = here - k
            back = jnp.where(back < 0, back + members, back)
            to = pl.ds(pl.multiple_of(back * each, each), each)
            for p in range(pieces):
                row_ref[:, to, p * LANES : (p + 1) * LANES] = ins[k][:, p * each : (p + 1) * each, :]
        named_rows = named_ref[...].astype(F32)
        one, two = [
            jnp.concatenate([named_rows[j, r : r + 1, :part] for j in range(n)], axis=0) for r in range(2)
        ]
        earlier = (iota((part, part), 0) < iota((part, part), 1)).astype(BF)
        slot = iota((capacity, part), 0).astype(F32)
        ranks = []
        for k in range(per_device):
            e = here * per_device + expert_at(k, per_device)
            hit = (one == e.astype(F32)) | (two == e.astype(F32))
            rank = dot(jnp.where(hit, 1.0, 0.0).astype(BF), earlier)
            ranks.append(jnp.where(hit, rank, -1.0))
        for j in range(n):
            pick = [jnp.where(slot == ranks[k][j : j + 1], 1.0, 0.0) for k in range(per_device)]
            got = dot(jnp.concatenate(pick, axis=0).astype(BF), row_ref[j]).astype(BF)
            for k in range(per_device):
                for p in range(pieces):
                    outs[k][j, p * capacity : (p + 1) * capacity, :] = got[
                        k * capacity : (k + 1) * capacity, p * LANES : (p + 1) * LANES
                    ]

    return pl.pallas_call(
        body,
        out_shape=tuple(held((n, pieces * capacity, LANES)) for _ in range(per_device)),
        in_specs=[VM] * (members + 1),
        out_specs=tuple(VM for _ in range(per_device)),
        compiler_params=LIMIT,
        scratch_shapes=[pltpu.VMEM((n, part, pieces * LANES), BF)],
    )(*near_core([*blocks, named]))


def expert_at(k, per_device):
    return (lax.axis_index("grp") + per_device - k) % per_device


def gather_tp(x, back):
    left, right = (shift(x, "tp_0", 1), shift(x, "tp_0", -1))
    across = shift(right, "tp_0", -1) if back else shift(left, "tp_0", 1)
    mine = (x, left, right, across)
    return mine + tuple(shift(b, "tp_1", 1) for b in mine)


def places_of():
    own, x = (lax.axis_index("tp_1"), lax.axis_index("tp_0"))
    return [
        ((x + ahead) % 4) * 2 + core for core in (own, 1 - own) for ahead in (0, 3, 1, 2)
    ]


def first_matmuls(blocks, gate, up, capacity):
    n, tall, _ = blocks[0].shape
    pieces = tall // capacity
    width = pieces * LANES
    depth, cols = gate.shape
    rows = n * capacity
    count = len(blocks)

    def body(*refs):
        ins, (gate_ref, up_ref, out_ref, in_buf, w_buf) = (refs[:count], refs[count:])
        for i, tp in enumerate(places_of()):
            d = pl.ds(pl.multiple_of(tp * width, width), width)
            to = slice(i * width, (i + 1) * width)
            w_buf[to, :cols] = gate_ref[d, :]
            w_buf[to, cols:] = up_ref[d, :]
            for p in range(pieces):
                lanes = slice(i * width + p * LANES, i * width + (p + 1) * LANES)
                in_buf[:, lanes] = ins[i][:, p * capacity : (p + 1) * capacity, :].reshape(rows, LANES)
        both = dot(in_buf[...], w_buf[...])
        g = both[:, :cols]
        out_ref[...] = (g / (1.0 + jnp.exp(-g)) * both[:, cols:]).astype(BF)

    return pl.pallas_call(
        body,
        out_shape=held((rows, cols)),
        in_specs=[VM] * (count + 2),
        out_specs=VM,
        compiler_params=LIMIT,
        scratch_shapes=[pltpu.VMEM((rows, depth), BF), pltpu.VMEM((depth, 2 * cols), BF)],
    )(*near_core([*blocks, gate, up]))


def second_matmul(blocks, down, n, k, per_device, done):
    rows, width = blocks[0].shape
    depth, cols = down.shape
    capacity = rows // n
    count = len(blocks)
    last = k == per_device - 1

    def body(*refs):
        ins, (down_ref, *dones) = (refs[:count], refs[count : count + 1 + len(done)])
        out_ref, in_buf, down_buf, *rest = refs[count + 1 + len(done) :]
        for i, tp in enumerate(places_of()):
            to = slice(i * width, (i + 1) * width)
            down_buf[to, :] = down_ref[pl.ds(pl.multiple_of(tp * width, width), width), :]
            in_buf[:, to] = ins[i][...]
        out = dot(in_buf[...], down_buf[...]).reshape(n, capacity, cols).astype(BF)
        if not last:
            out_ref[...] = out
            return
        row_ref, sems = rest
        copies = [
            pltpu.make_async_copy(ref, out_ref.at[:, expert_at(i, per_device)], sems.at[i])
            for i, ref in enumerate((*dones, row_ref))
        ]
        for c in copies[:-1]:
            c.start()
        row_ref[...] = out
        copies[-1].start()
        for c in copies:
            c.wait()

    return pl.pallas_call(
        body,
        out_shape=pltpu.HBM((n, per_device, capacity, cols), BF) if last else held((n, capacity, cols)),
        in_specs=[VM] * (count + 1 + len(done)),
        out_specs=pl.BlockSpec(memory_space=pltpu.HBM) if last else VM,
        compiler_params=LIMIT,
        scratch_shapes=[pltpu.VMEM((rows, depth), BF), pltpu.VMEM((depth, cols), BF)]
        + [pltpu.VMEM((n, capacity, cols), BF), pltpu.SemaphoreType.DMA((per_device,))] * last,
    )(*near_core([*blocks, down, *done]))


def weigh(route_ids, route_weights, slots, capacity):
    rows = route_ids.shape[0]

    def body(ids_ref, w_ref, out_ref):
        lane = iota((rows, slots), 1)
        total = jnp.zeros((rows, slots), F32)
        for r, slot in enumerate(slot_of(ids_ref, capacity)):
            total = jnp.where(lane == slot, as_column(w_ref[r : r + 1, :]), total)
        high = total.astype(BF)
        out_ref[0] = high
        out_ref[1] = (total - high.astype(F32)).astype(BF)

    return pl.pallas_call(
        body,
        out_shape=held((2, rows, slots)),
        in_specs=[VM] * 2,
        out_specs=VM,
        compiler_params=LIMIT,
    )(route_ids.T, route_weights.T)


def combine(returned, picks):
    def body(ret_ref, pick_ref, out_ref):
        rows = ret_ref[...].reshape(-1, ret_ref.shape[-1])
        out_ref[...] = (dot(pick_ref[0], rows) + dot(pick_ref[1], rows)).astype(BF)

    return pl.pallas_call(
        body,
        out_shape=shape((picks.shape[1], returned.shape[-1])),
        in_specs=[VM] * 2,
        out_specs=VM,
        compiler_params=LIMIT,
    )(*near_core([returned, picks]))


def by_target(master, n):
    return master.reshape(n, -1, master.shape[2])


def share(master, index, count, n):
    whole = by_target(master, n)
    size = whole.shape[1] // count
    return lax.dynamic_slice_in_dim(whole, index * size, size, 1)


def ring(x, axis):
    n = lax.axis_size(axis)
    out, ahead, behind = ([(0, x)], x, x)
    for k in range(1, n // 2 + 1):
        ahead = shift(ahead, axis, 1)
        out.append((k, ahead))
        if k <= (n - 1) // 2:
            behind = shift(behind, axis, -1)
            out.append((n - k, behind))
    return out


def assemble(pieces, index, count, per_device):
    n, rows, cols = pieces[0][1].shape
    buffer = jnp.zeros((count, n, rows, cols), BF)
    for back, piece in pieces:
        at = (index - back) % count
        buffer = lax.dynamic_update_slice(buffer, piece[None], (at, 0, 0, 0))
    split = count // per_device
    buffer = buffer.reshape(per_device, split, n, rows, cols).transpose(0, 2, 1, 3, 4)
    return buffer.reshape(per_device, -1, cols)


def one_by_one(pieces, served, index, count, per_device):
    if count == per_device:
        return [p.reshape(-1, p.shape[-1]) for _, p in sorted(pieces, key=lambda q: q[0])]
    return [
        lax.dynamic_index_in_dim(served, (index + per_device - k) % per_device, 0, False)
        for k in range(per_device)
    ]


def on_device(tokens, route_ids, route_weights, ffn_gain, gate_master, up_master, down_master):
    n = lax.axis_size("fs")
    count, index = (lax.axis_size("grp"), lax.axis_index("grp"))
    experts, rows, _ = gate_master.shape
    per_device = experts // n
    groups = experts // GROUP_SIZE
    members = n // groups
    capacity = tokens.shape[0] // (2 * groups)
    size = per_device * rows // count

    def swap(x):
        return lax.all_to_all(x, "fs", split_axis=0, concat_axis=0, tiled=True)

    def neighbour(x, k):
        pairs = [(i, i - i % members + (i + k) % members) for i in range(n)]
        return lax.ppermute(x, "fs", pairs)

    packed = pack_first(
        tokens, route_ids, ffn_gain[None, :], by_target(gate_master, n), n, count, groups
    )
    packed = swap(packed)
    gate, near, named = jnp.split(packed, [size, packed.shape[1] - META], axis=1)
    near = [near] + [neighbour(near, k) for k in range(1, members)]
    if size < rows:
        gain = lax.dynamic_slice_in_dim(ffn_gain, index * size % rows, size)
    else:
        gain = jnp.concatenate([ffn_gain] * (size // rows))
    up = swap((share(up_master, index, count, n) * gain[None, :, None]).astype(BF))
    chosen = select_rows(near, named, per_device, capacity)
    down = swap(share(down_master, index, count, n).astype(BF))
    gate = ring(gate, "grp")
    up = ring(up, "grp")
    down = ring(down, "grp")
    gate_serve = assemble(gate, index, count, per_device)
    up_serve = assemble(up, index, count, per_device)
    down_serve = assemble(down, index, count, per_device)
    gates = one_by_one(gate, gate_serve, index, count, per_device)
    ups = one_by_one(up, up_serve, index, count, per_device)
    downs = one_by_one(down, down_serve, index, count, per_device)
    outs = []
    for k in range(per_device):
        blocks = gather_tp(chosen[k], k % 2)
        hidden = first_matmuls(blocks, gates[k], ups[k], capacity)
        hidden = gather_tp(hidden, k % 2)
        last = k == per_device - 1
        outs.append(second_matmul(hidden, downs[k], n, k, per_device, outs if last else []))
    picks = weigh(route_ids, route_weights, experts * capacity, capacity)
    out = swap(outs[-1])
    mixed = combine(out, picks)
    return (gate_serve, up_serve, down_serve, mixed)


def solution(mesh):
    grp, fs, tp = (mesh.shape["grp"], mesh.shape["fs"], mesh.shape["tp"])
    split = Mesh(mesh.devices.reshape(grp, fs, tp // 2, 2), ("grp", "fs", *TP))
    in_specs = (
        P(("grp", "fs"), None),
        P(("grp", "fs"), None),
        P(("grp", "fs"), None),
        P("fs"),
        P(None, "fs", TP),
        P(None, "fs", TP),
        P(None, "fs", TP),
    )
    out_specs = (
        P(("grp", "fs"), None, TP),
        P(("grp", "fs"), None, TP),
        P(("grp", "fs"), None, TP),
        P(("grp", "fs"), TP),
    )
    return jax.shard_map(on_device, mesh=split, in_specs=in_specs, out_specs=out_specs, check_vma=False)
```
